128 devices in a mesh: sp: 32 (over z, y, core), tp: 4 (over x).
Axes of the slice: x: 4, y: 4, z: 4, core: 2. Of those that a mesh axis runs over, the one named last changes fastest.
Arguments:
- queries: bfloat16 [16384, 512], P('sp', 'tp'), may hold values from -6 to 6
- key_matrix: bfloat16 [16384, 512], P('sp', 'tp'), may hold values from -6 to 6
- value_matrix: bfloat16 [16384, 1024], P('sp', 'tp'), may hold values from -6 to 6
- channel_decay_input: bfloat16 [16384, 512], P('sp', 'tp')
- head_decay_offset: float32 [16384, 8], P('sp', 'tp'), may hold values from -1 to 0
- output_gate_input: bfloat16 [16384, 1024], P('sp', 'tp'), may hold values from -6 to 6
- head_norm_gain: float32 [128], replicated, may hold values from 0.1 to 1.9
- residual: bfloat16 [16384, 2048], P(('sp', 'tp')), may hold values from -6 to 6
- mixer_output_weight: bfloat16 [1024, 2048], replicated, may hold values from -0.1875 to 0.1875
- expert_norm_gain: float32 [2048], replicated, may hold values from 0.1 to 1.9
- routes: int32 [16384, 4], P(('sp', 'tp')), may hold values from 0 to 255, all different within a row; in each aligned block of 128 rows (0 to 127, 128 to 255, ...) at most 4 rows name the same one
- chosen_router_scores: float32 [16384, 4], P(('sp', 'tp')), may hold values from 0.1 to 1
- routed_gate_weight: bfloat16 [256, 2048, 512], P(('sp', 'tp')), may hold values from -0.125 to 0.125
- routed_up_weight: bfloat16 [256, 2048, 512], P(('sp', 'tp')), may hold values from -0.125 to 0.125
- routed_down_weight: bfloat16 [256, 512, 2048], P(('sp', 'tp')), may hold values from -0.25 to 0.25
- common_gate_weight: bfloat16 [2048, 512], replicated, may hold values from -0.125 to 0.125
- common_up_weight: bfloat16 [2048, 512], replicated, may hold values from -0.125 to 0.125
- common_down_weight: bfloat16 [512, 2048], replicated, may hold values from -0.25 to 0.25
Outputs:
- layer_out: bfloat16 [16384, 2048], P(('sp', 'tp'))
The draws below stay inside these ranges and needn't reach their ends.
Inputs may be any that keep to these rules, and one draw needn't show every extreme that they name: `routes`: each row names 4 different experts. In each aligned block of 128 rows (the rows of one device) no expert is named by more than 4 rows, a bound that some block reaches.
All inputs are finite; a program needn't handle non-finite values.
Results may differ from the reference program's by a relative error of at most 0.017.
Values may be sent and summed in bfloat16 or wider, within the bound.
A program may use at most 128 MiB of HBM per device.

```python
import math
import jax
import jax.numpy as jnp
import numpy as np
from jax import lax

D = 2048
HEADS = 8
KEY_CHANNELS = 64
VDIM = 128
BLOCK = 64
FFE = 512
SFF = 512
TOP_K = 4
TOK_DEV = 128
KW = 512
VW = 1024
TOK_SP = 512
TOKENS = 16384
EXPERTS = 256
CAP = 4


def draw_channel_decay_input(key, part):
    head_key = jax.random.fold_in(key, 11)
    channel_key = jax.random.fold_in(key, 12)
    shift_key = jax.random.fold_in(key, 13)
    jitter_key = jax.random.fold_in(key, 14)
    slow_heads = jax.random.bernoulli(head_key, 0.5, (HEADS,))
    jitter = jnp.clip(0.5 * jax.random.normal(jitter_key, (TOKENS, HEADS * KEY_CHANNELS), jnp.float32), -1.5, 1.5)
    head_base = jnp.where(slow_heads, math.log(TOKENS) - 1.5, 0.5).astype(jnp.float32)
    channel = jax.random.uniform(channel_key, (HEADS, KEY_CHANNELS), jnp.float32, -0.5, 0.5)
    column = (head_base[:, None] + channel).reshape(HEADS * KEY_CHANNELS)
    shifts = jax.random.uniform(shift_key, (TOKENS // TOK_SP,), jnp.float32, 0.0, math.log(4.0))
    rows_shift = jnp.repeat(shifts, TOK_SP)
    return (column[None, :] + jitter - rows_shift[:, None]).astype(jnp.bfloat16)


def draw_head_decay_offset(key, part):
    place_key = jax.random.fold_in(key, 21)
    size_key = jax.random.fold_in(key, 22)
    places = jax.random.randint(place_key, (3, HEADS), 0, TOKENS)
    drops = jax.random.uniform(size_key, (3, HEADS), jnp.float32, math.log(0.5), math.log(0.8))
    positions = jnp.arange(TOKENS, dtype=jnp.int32)
    landed = positions[:, None, None] == places[None, :, :]
    return jnp.sum(jnp.where(landed, drops[None, :, :], 0.0), axis=1).astype(jnp.float32)


def level_of(own_key, shape, shards, low, high):
    def one(position, blocks):
        heights = jax.random.uniform(jax.random.fold_in(jax.random.fold_in(own_key, 6), position), (blocks,), jnp.float32, low / len(shards), high / len(shards))
        return jnp.repeat(jnp.exp(heights), shape[position] // blocks).reshape((-1,) + (1,) * (len(shape) - position - 1))

    loudness = one(*shards[0])
    for cut in shards[1:]:
        loudness = loudness * one(*cut)
    return loudness


def routed_block(stream_key, own, number, rows, number_of, top, reach, skew):
    order = jax.random.permutation(stream_key, number_of)
    heavy_load, ordinary = portions_of(number_of, rows * top, reach, skew, True), portions_of(number_of, rows * top, reach, skew, False)
    places = jnp.arange(number_of)

    def named(sizes, offset_by):
        used = int((sizes > 0).sum())
        fixed = max(1, used // 4)
        passed = fixed + (places - fixed + offset_by * (used - fixed)) % max(1, number_of - fixed)
        return jnp.zeros((number_of,), jnp.int32).at[order[jnp.where(places < fixed, places, passed)]].set(jnp.asarray(sizes, jnp.int32))

    sizes = jnp.where(number % 4 == 0, named(heavy_load, number // 4), named(ordinary, number - number // 4 - 1))
    mixed = jax.random.permutation(jax.random.fold_in(own, 3), number_of)
    giver, taker = mixed[0:number_of // 2 * 2:2], mixed[1:number_of // 2 * 2:2]
    margin = jnp.minimum(sizes[giver] - 1, reach - sizes[taker]) // 2
    margin = jnp.where((giver == order[0]) | (taker == order[0]) | (sizes[taker] == 0), 0, jnp.maximum(margin, 0))
    passed = jax.random.randint(jax.random.fold_in(own, 4), (number_of // 2,), 0, 1 << 20) % (margin + 1)
    sizes = sizes.at[giver].add(-passed).at[taker].add(passed)
    items = jnp.searchsorted(jnp.cumsum(sizes), jnp.arange(rows * top), side="right").astype(jnp.int32)
    listing = items.reshape(top, rows).T
    listing = listing[jax.random.permutation(jax.random.fold_in(own, 1), rows)]
    offset_by = jax.random.randint(jax.random.fold_in(own, 2), (rows, 1), 0, top)
    return jnp.take_along_axis(listing, (jnp.arange(top)[None, :] + offset_by) % top, axis=1)


def portions_of(amount, total, reach, skew, full):
    portions = [(1 << 20) // math.isqrt(grade ** skew) + 1 for grade in range(1, amount + 1)]
    largest = reach if full else min(reach, max(-(-total // amount), total * portions[0] // sum(portions)))
    least = 1 if total - largest >= amount - 1 else 0
    given, surplus = [largest] + [least] * (amount - 1), total - largest - least * (amount - 1)
    while surplus > 0:
        movable = [i for i in range(1, amount) if given[i] < largest] or [i for i in range(1, amount) if given[i] < reach]
        mass, budget = sum([portions[i] for i in movable]), surplus
        for i in movable:
            extra = min(reach - given[i], max(1, budget * portions[i] // mass), surplus)
            given[i] = given[i] + extra
            surplus = surplus - extra
    return np.array(given)


def scatter_about(own_key, shape, deviation, reach, cuts=(), held_as=jnp.bfloat16):
    values = jax.random.normal(own_key, shape, jnp.float32) * deviation
    if len(cuts) > 0:
        values = level_of(own_key, shape, cuts, -0.22, 0.18) * values
    return jnp.clip(values, min=-reach, max=reach).astype(held_as)


def setup_inputs(seed: int = 0) -> dict:
    arg_keys = jax.random.split(jax.random.key(seed), 19)
    queries = scatter_about(arg_keys[0], (TOKENS, KW), 1.0, 6.0, ((0, 32), (1, 4)))
    key_matrix = scatter_about(arg_keys[1], (TOKENS, KW), 1.0, 6.0, ((0, 32), (1, 4)))
    value_matrix = scatter_about(arg_keys[2], (TOKENS, VW), 1.0, 6.0, ((0, 32), (1, 4)))
    channel_decay_input = draw_channel_decay_input(jax.random.fold_in(arg_keys[18], 71), 0)
    head_decay_offset = draw_head_decay_offset(jax.random.fold_in(arg_keys[18], 71), 0)
    output_gate_input = scatter_about(arg_keys[5], (TOKENS, VW), 1.0, 6.0, ((0, 32), (1, 4)))
    head_norm_gain = jnp.clip(1.0 + 0.18 * jax.random.normal(arg_keys[6], (VDIM,), jnp.float32), 0.1, 1.9)
    residual = scatter_about(arg_keys[7], (TOKENS, D), 1.0, 6.0, ((0, 128),))
    mixer_output_weight = scatter_about(arg_keys[8], (VW, D), VW ** -0.5, 0.1875)
    expert_norm_gain = jnp.clip(1.0 + 0.18 * jax.random.normal(arg_keys[9], (D,), jnp.float32), 0.1, 1.9)
    routes_keys = jax.random.split(jax.random.fold_in(arg_keys[10], 1), TOKENS // TOK_DEV)
    routes_turns = jax.random.permutation(jax.random.fold_in(arg_keys[10], 3), TOKENS // TOK_DEV)
    routes = jax.vmap(lambda own, number: routed_block(jax.random.fold_in(arg_keys[10], 2), own, number, TOK_DEV, EXPERTS, TOP_K, CAP, 2))(routes_keys, routes_turns).reshape((TOKENS, TOP_K))
    chosen_router_scores = jnp.clip(jnp.exp(math.log(1.0) - 2.3025851 * jax.random.uniform(arg_keys[11], (TOKENS, TOP_K), jnp.float32) ** level_of(arg_keys[11], (TOKENS, TOP_K), ((0, 128),), -0.2, 0.2)), 0.1, 1.0)
    routed_gate_weight = scatter_about(arg_keys[12], (EXPERTS, D, FFE), D ** -0.5, 0.125, ((0, 128),))
    routed_up_weight = scatter_about(arg_keys[13], (EXPERTS, D, FFE), D ** -0.5, 0.125, ((0, 128),))
    routed_down_weight = scatter_about(arg_keys[14], (EXPERTS, FFE, D), FFE ** -0.5, 0.25, ((0, 128),))
    common_gate_weight = scatter_about(arg_keys[15], (D, SFF), D ** -0.5, 0.125)
    common_up_weight = scatter_about(arg_keys[16], (D, SFF), D ** -0.5, 0.125)
    common_down_weight = scatter_about(arg_keys[17], (SFF, D), SFF ** -0.5, 0.25)
    return dict(queries=queries, key_matrix=key_matrix, value_matrix=value_matrix, channel_decay_input=channel_decay_input, head_decay_offset=head_decay_offset, output_gate_input=output_gate_input, head_norm_gain=head_norm_gain, residual=residual, mixer_output_weight=mixer_output_weight, expert_norm_gain=expert_norm_gain, routes=routes, chosen_router_scores=chosen_router_scores, routed_gate_weight=routed_gate_weight, routed_up_weight=routed_up_weight, routed_down_weight=routed_down_weight, common_gate_weight=common_gate_weight, common_up_weight=common_up_weight, common_down_weight=common_down_weight)


eps_norm = 1e-06
decay_running = 16.0
routed_scale = 2.5

def split_heads(values, columns):
    blocks = values.shape[0] // BLOCK
    return values.astype(jnp.float32).reshape(blocks, BLOCK, HEADS, columns).transpose(2, 0, 1, 3)

def recurrent_mixer(queries, key_matrix, value_matrix, channel_decay_input, head_decay_offset, output_gate_input, head_norm_gain):
    decay_spike_columns = jnp.repeat(head_decay_offset, KEY_CHANNELS, axis=1)
    decay_logarithm = jax.nn.log_sigmoid(channel_decay_input.astype(jnp.float32)) / decay_running + decay_spike_columns
    within = jnp.cumsum(split_heads(decay_logarithm, KEY_CHANNELS), axis=2)
    block_end = within[:, :, -1:, :]
    q_heads = split_heads(queries, KEY_CHANNELS) * KEY_CHANNELS ** (-0.5)
    k_heads = split_heads(key_matrix, KEY_CHANNELS)
    v_heads = split_heads(value_matrix, VDIM)
    q_decay = q_heads * jnp.exp(within)
    k_grow = k_heads * jnp.exp(-within)
    k_tail = k_heads * jnp.exp(block_end - within)
    causal = jnp.tril(jnp.ones((BLOCK, BLOCK), dtype=bool))
    scores = jnp.where(causal, jnp.einsum('hnid,hnjd->hnij', q_decay, k_grow), 0.0)
    output = jnp.einsum('hnij,hnje->hnie', scores, v_heads)
    block_state = jnp.einsum('hncd,hnce->nhde', k_tail, v_heads)
    block_decay = jnp.moveaxis(jnp.exp(block_end[:, :, 0, :]), 1, 0)

    def advance(carried, block_inputs):
        added_state, factor = block_inputs
        return (factor[..., None] * carried + added_state, carried)
    start_state = jnp.zeros((HEADS, KEY_CHANNELS, VDIM), jnp.float32)
    _, entering = lax.scan(advance, start_state, (block_state, block_decay))
    output = output + jnp.einsum('hncd,nhde->hnce', q_decay, entering)
    output = output.transpose(1, 2, 0, 3).reshape(-1, HEADS, VDIM)
    inv_rms = lax.rsqrt(lax.optimization_barrier(jnp.mean(output * output, axis=-1, keepdims=True)) + eps_norm)
    normed = (output * inv_rms * head_norm_gain).reshape(-1, HEADS * VDIM)
    return (normed * jax.nn.silu(output_gate_input.astype(jnp.float32))).astype(jnp.bfloat16)

def expert_block(picked_rows, gate_weight, up_weight, down_weight):
    gate_pre = jnp.dot(picked_rows, gate_weight, preferred_element_type=jnp.float32)
    up_pre = jnp.dot(picked_rows, up_weight, preferred_element_type=jnp.float32)
    hidden = (jax.nn.silu(gate_pre) * up_pre).astype(jnp.bfloat16)
    return jnp.dot(hidden, down_weight, preferred_element_type=jnp.float32)

def reference(queries, key_matrix, value_matrix, channel_decay_input, head_decay_offset, output_gate_input, head_norm_gain, residual, mixer_output_weight, expert_norm_gain, routes, chosen_router_scores, routed_gate_weight, routed_up_weight, routed_down_weight, common_gate_weight, common_up_weight, common_down_weight):
    gated_output = recurrent_mixer(queries, key_matrix, value_matrix, channel_decay_input, head_decay_offset, output_gate_input, head_norm_gain)
    middle = (residual.astype(jnp.float32) + jnp.dot(gated_output, mixer_output_weight, preferred_element_type=jnp.float32)).astype(jnp.bfloat16)
    middle_wide = middle.astype(jnp.float32)
    inv_rms = lax.rsqrt(lax.optimization_barrier(jnp.mean(middle_wide * middle_wide, axis=-1, keepdims=True)) + eps_norm)
    normed = (middle_wide * inv_rms * expert_norm_gain).astype(jnp.bfloat16)
    weights = routed_scale * chosen_router_scores / lax.optimization_barrier(jnp.sum(chosen_router_scores, axis=-1, keepdims=True))
    flat_expert = routes.reshape(-1).astype(jnp.int32)
    assigned = TOKENS * TOP_K
    flat_token = (jnp.arange(assigned, dtype=jnp.int32) // TOP_K).astype(jnp.int32)
    flat_weight = weights.reshape(-1)
    sorted_ids = jnp.argsort(flat_expert, stable=True).astype(jnp.int32)
    counts = jnp.bincount(flat_expert, length=EXPERTS).astype(jnp.int32)
    starts = (jnp.cumsum(counts) - counts).astype(jnp.int32)
    slot_room = TOKENS // TOK_DEV * CAP
    order_pad = jnp.concatenate([sorted_ids, jnp.full((slot_room,), assigned, jnp.int32)])
    token_pad = jnp.concatenate([flat_token, jnp.full((1,), TOKENS, jnp.int32)])
    weight_pad = jnp.concatenate([flat_weight, jnp.zeros((1,), jnp.float32)])
    normed_pad = jnp.concatenate([normed, jnp.zeros((1, D), jnp.bfloat16)], axis=0)

    def one_expert(summed, expert_id):
        picked = lax.dynamic_slice_in_dim(order_pad, starts[expert_id], slot_room)
        live_slot = jnp.arange(slot_room, dtype=jnp.int32) < counts[expert_id]
        picked = jnp.where(live_slot, picked, assigned).astype(jnp.int32)
        tokens = token_pad[picked]
        picked_rows = normed_pad[tokens]
        result = expert_block(picked_rows, routed_gate_weight[expert_id], routed_up_weight[expert_id], routed_down_weight[expert_id]).astype(jnp.bfloat16)
        return (summed.at[tokens].add(weight_pad[picked][:, None] * result.astype(jnp.float32)), None)
    routed, _ = lax.scan(one_expert, jnp.zeros((TOKENS + 1, D), jnp.float32), jnp.arange(EXPERTS, dtype=jnp.int32))
    shared = expert_block(normed, common_gate_weight, common_up_weight, common_down_weight)
    return (middle_wide + routed[:TOKENS] + shared).astype(jnp.bfloat16)
```

```python
import jax
import jax.numpy as jnp
from jax import lax
from jax.experimental import pallas as pl
from jax.experimental.pallas import tpu as pltpu
from jax.sharding import PartitionSpec as P

MESH = pl.DeviceIdType.MESH
BF = jnp.bfloat16
F32 = jnp.float32
I32 = jnp.int32

BLOCK = 64
NZ, NY, NC, NX = 4, 4, 2, 4
DEVS = NZ * NY * NC * NX
STRIDE = 37
CHUNK = 32
CHUNKS = DEVS // CHUNK

EPS = 1e-6
RUNNING = 16.0
SCALE = 2.5


def dot(a, b):
    return jnp.dot(a, b, preferred_element_type=F32)


def dot_nt(a, b):
    return lax.dot_general(a, b, (((1,), (1,)), ((), ())), preferred_element_type=F32)


def dot_tn(a, b):
    return lax.dot_general(a, b, (((0,), (0,)), ((), ())), preferred_element_type=F32)


def silu(v):
    return v / (1.0 + jnp.exp(-v))


def three(v):
    hi = v.astype(BF)
    rest = v - hi.astype(F32)
    mid = rest.astype(BF)
    low = (rest - mid.astype(F32)).astype(BF)
    return hi, mid, low


def kernel(
    q_hbm, k_hbm, v_hbm, cd_hbm, hd_ref, og_hbm, hgain_ref, res_hbm, wo_hbm, egain_ref,
    routes_ref, scores_ref, wg_hbm, wu_hbm, wd_hbm, cg_hbm, cu_hbm, cdn_hbm,
    out_ref,
    q_s, k_s, v_s, cd_s, og_s, res_s, wo_s, wg_s, wu_s, wd_s, cg_s, cu_s, cdn_s,
    st1, st1r, st2, st3, outacc, qx_s, gsend, grecv, mid_s, nrm_s, shared_s,
    lhs_s, cw_s, send, recv, ret, back, acc_s,
    load_sem, s1, r1, s2, r2, s3, r3, gs, gr, ds, dr, es, er,
):
    sp = lax.axis_index("sp")
    x = lax.axis_index("tp")
    z = sp // (NY * NC)
    y = (sp // NC) % NY
    c = sp % NC

    def place(zz, yy, cc, xx):
        return ((zz % NZ) * (NY * NC) + (yy % NY) * NC + cc % NC, xx % NX)

    loads = [
        pltpu.make_async_copy(a, b, load_sem.at[n])
        for n, (a, b) in enumerate(
            (
                (cd_hbm, cd_s), (k_hbm, k_s), (v_hbm, v_s), (q_hbm, q_s), (og_hbm, og_s),
                (wo_hbm, wo_s), (res_hbm, res_s), (cg_hbm, cg_s), (cu_hbm, cu_s),
                (cdn_hbm, cdn_s), (wg_hbm, wg_s), (wu_hbm, wu_s), (wd_hbm, wd_s),
            )
        )
    ]
    for one in loads:
        one.start()
    (l_cd, l_k, l_v, l_q, l_og, l_wo, l_res, l_cg, l_cu, l_cdn, l_wg, l_wu, l_wd) = loads

    bar = pltpu.get_barrier_semaphore()
    neighbours = [place(z, y, c + 1, x)]
    neighbours += [place(z, y + d, c, x) for d in (1, 2, 3)]
    neighbours += [place(z + d, y, c, x) for d in (1, 2, 3)]
    neighbours += [place(z, y, c, x + d) for d in (1, 2, 3)]
    for one in neighbours:
        pl.semaphore_signal(bar, inc=1, device_id=one, device_id_type=MESH)

    lane = lax.broadcasted_iota(I32, (1, 128), 1)
    first = lane < 64
    rows_i = lax.broadcasted_iota(I32, (256, 256), 0)
    cols_i = lax.broadcasted_iota(I32, (256, 256), 1)
    causal = (rows_i >= cols_i) & ((rows_i >> 6) == (cols_i >> 6))
    tri = causal.astype(F32).astype(BF)
    hd = jnp.where(first, hd_ref[:, 0:1], hd_ref[:, 1:2])
    l_cd.wait()
    cd = cd_s[...].astype(F32)
    dl = (jnp.minimum(cd, 0.0) - jnp.log1p(jnp.exp(-jnp.abs(cd)))) / RUNNING + hd
    parts = three(dl)
    within = jnp.concatenate(
        [sum(dot(tri, p[256 * n : 256 * n + 256]) for p in parts) for n in (0, 1)], axis=0
    )
    w3 = within.reshape(8, BLOCK, 128)
    ends = [w3[n, BLOCK - 1 : BLOCK, :] for n in range(8)]
    incl = []
    running = jnp.zeros((1, 128), F32)
    for n in range(8):
        running = running + ends[n]
        incl.append(running)
    total = incl[7]
    excl3 = jnp.stack([incl[n] - ends[n] for n in range(8)], axis=0)
    ends3 = jnp.stack(ends, axis=0)

    l_k.wait()
    l_v.wait()
    k = k_s[...].astype(F32)
    k3 = k.reshape(8, BLOCK, 128)
    k_tt = (k3 * jnp.exp(total[None] - excl3 - w3)).reshape(512, 128).astype(BF)
    v0, v1 = v_s[:, 0:128], v_s[:, 128:256]
    own_state = jnp.where(first, dot_tn(v0, k_tt), dot_tn(v1, k_tt))

    row16 = lax.broadcasted_iota(I32, (16, 128), 0)

    def put_state(ref, log, state):
        ref[0:128, :] = state.astype(BF)
        hi, mid, low = (p.astype(F32) for p in three(log))
        tail = jnp.where(row16 == 0, hi, jnp.where(row16 == 1, mid, jnp.where(row16 == 2, low, 0.0)))
        ref[128:144, :] = tail.astype(BF)

    def get_state(ref):
        log = jnp.sum(ref[128:144, :].astype(F32), axis=0, keepdims=True)
        return log, ref[0:128, :].astype(F32)

    put_state(st1, total, own_state)
    pl.semaphore_wait(bar, 10)
    core_copy = pltpu.make_async_remote_copy(
        src_ref=st1, dst_ref=st1r, send_sem=s1, recv_sem=r1,
        device_id=place(z, y, c + 1, x), device_id_type=MESH,
    )
    core_copy.start()

    l_q.wait()
    ew = jnp.exp(within)
    qd = q_s[...].astype(F32) * 0.125 * ew
    qx_s[...] = (qd.reshape(8, BLOCK, 128) * jnp.exp(excl3)).reshape(512, 128).astype(BF)
    kg = (k * jnp.exp(-within)).astype(BF)
    for h in (0, 1):
        q_h = jnp.where(first if h == 0 else ~first, qd, 0.0).astype(BF)
        v_h = v0 if h == 0 else v1
        for n in (0, 1):
            sl = slice(256 * n, 256 * n + 256)
            scores = jnp.where(causal, dot_nt(q_h[sl], kg[sl]), 0.0).astype(BF)
            outacc[h, sl, :] = dot(scores, v_h[sl])

    core_copy.wait()
    core1 = c == 1
    log_p, state_p = get_state(st1r)
    pair_log = total + log_p
    pair_state = jnp.where(
        core1,
        jnp.exp(total) * state_p + own_state,
        jnp.exp(log_p) * own_state + state_p,
    )
    carry_log = jnp.where(core1, log_p, 0.0)
    carry_state = jnp.where(core1, state_p, 0.0)

    def exchange(slots, mine, log, state, ssem, rsem, target):
        put_state(slots.at[mine], log, state)
        copies = []
        for d in (1, 2, 3):
            one = pltpu.make_async_remote_copy(
                src_ref=slots.at[mine], dst_ref=slots.at[mine],
                send_sem=ssem.at[d], recv_sem=rsem.at[d],
                device_id=target(d), device_id_type=MESH,
            )
            one.start()
            copies.append(one)
        return copies

    def prefix(slots, mine, count, carry_log, carry_state):
        run_log = jnp.zeros((1, 128), F32)
        run_state = jnp.zeros((128, 128), F32)
        pre_log, pre_state = run_log, run_state
        for n in range(count):
            pre_log = jnp.where(mine == n, run_log, pre_log)
            pre_state = jnp.where(mine == n, run_state, pre_state)
            log, state = get_state(slots.at[n])
            run_state = jnp.exp(log) * run_state + state
            run_log = run_log + log
        carry_state = jnp.exp(carry_log) * pre_state + carry_state
        carry_log = carry_log + pre_log
        return run_log, run_state, carry_log, carry_state

    y_copies = exchange(st2, y, pair_log, pair_state, s2, r2, lambda d: place(z, y + d, c, x))

    k_tail = (k3 * jnp.exp(ends3 - w3)).reshape(512, 128).astype(BF)
    state = jnp.zeros((128, 128), F32)
    for n in range(8):
        sl = slice(BLOCK * n, BLOCK * n + BLOCK)
        if n > 0:
            state_b = state.astype(BF)
            for h in (0, 1):
                q_h = jnp.where(first if h == 0 else ~first, qd[sl], 0.0).astype(BF)
                outacc[h, sl, :] += dot_nt(q_h, state_b)
        if n < 7:
            added = jnp.where(first, dot_tn(v0[sl], k_tail[sl]), dot_tn(v1[sl], k_tail[sl]))
            state = jnp.exp(ends[n]) * state + added

    for one in y_copies:
        one.wait()
    plane_log, plane_state, carry_log, carry_state = prefix(st2, y, NY, carry_log, carry_state)
    z_copies = exchange(st3, z, plane_log, plane_state, s3, r3, lambda d: place(z + d, y, c, x))

    def expert_of(index):
        off = ((index >> 4) * STRIDE) & (DEVS - 1)
        dev = ((z + (off >> 5)) & 3) * 8 + ((y + (off >> 3)) & 3) * 2 + ((c + off) & 1)
        return (dev * 4 + ((x + (off >> 1)) & 3)) * 2 + ((index >> 2) & 1)

    routes = routes_ref[...].astype(F32)
    sub128 = lax.broadcasted_iota(I32, (128, 128), 0)
    lan128 = lax.broadcasted_iota(I32, (128, 128), 1)
    upper = (sub128 < lan128).astype(F32).astype(BF)
    lower = (sub128 > lan128).astype(F32).astype(BF)
    wide = jnp.zeros((128, 128), F32)
    for n in range(4):
        wide = jnp.where(lan128 == n, routes[:, n : n + 1], wide)
    turned = wide.T
    for n in range(8):
        q_index = lax.broadcasted_iota(I32, (256, 128), 0) + 256 * n
        expert = expert_of(q_index).astype(F32)
        match = jnp.zeros((256, 128), F32)
        for j in range(4):
            match = jnp.where(expert == turned[j : j + 1, :], 1.0, match)
        rank = dot(match.astype(BF), upper)
        live = jnp.where(rank == (q_index & 3).astype(F32), match, 0.0)
        half = ((q_index >> 3) & 1) == 0
        lhs_s[256 * n : 256 * n + 256, 0:128] = jnp.where(half, live, 0.0).astype(BF)
        lhs_s[256 * n : 256 * n + 256, 128:256] = jnp.where(half, 0.0, live).astype(BF)
    scores = scores_ref[...]
    weights = SCALE * scores / jnp.sum(scores, axis=-1, keepdims=True)
    for n in range(4):
        q_index = lax.broadcasted_iota(I32, (128, 512), 1) + 512 * n
        expert = expert_of(q_index).astype(F32)
        weight = jnp.zeros((128, 512), F32)
        match = jnp.zeros((128, 512), F32)
        for j in range(4):
            hit = expert == routes[:, j : j + 1]
            match = jnp.where(hit, 1.0, match)
            weight = jnp.where(hit, weights[:, j : j + 1], weight)
        rank = dot(lower, match.astype(BF))
        weight = jnp.where(rank == (q_index & 3).astype(F32), weight, 0.0)
        half = ((q_index >> 3) & 1) == 0
        cw_s[0:128, 512 * n : 512 * n + 512] = jnp.where(half, weight, 0.0).astype(BF)
        cw_s[128:256, 512 * n : 512 * n + 512] = jnp.where(half, 0.0, weight).astype(BF)

    for one in z_copies:
        one.wait()
    _, _, _, carried = prefix(st3, z, NZ, carry_log, carry_state)
    carried_b = carried.astype(BF)

    l_og.wait()
    g_copies = []
    for d in (1, 2, 3, 0):
        xx = (x + d) % NX
        rows = pl.ds(pl.multiple_of(xx * 128, 128), 128)
        qx = qx_s[rows, :]
        for h in (0, 1):
            q_h = jnp.where(first if h == 0 else ~first, qx.astype(F32), 0.0).astype(BF)
            attn = outacc[h, rows, :] + dot_nt(q_h, carried_b)
            inv = lax.rsqrt(jnp.mean(attn * attn, axis=-1, keepdims=True) + EPS)
            gate = og_s[rows, 128 * h : 128 * h + 128].astype(F32)
            value = attn * inv * hgain_ref[...] * silu(gate)
            gsend[d, :, 128 * h : 128 * h + 128] = value.astype(BF)
        if d > 0:
            one = pltpu.make_async_remote_copy(
                src_ref=gsend.at[d], dst_ref=grecv.at[d], send_sem=gs.at[d], recv_sem=gr.at[d],
                device_id=place(z, y, c, x + d), device_id_type=MESH,
            )
            one.start()
            g_copies.append(one)

    l_wo.wait()
    l_res.wait()
    w_rows = pl.ds(pl.multiple_of(x * 256, 256), 256)
    proj = dot(gsend[0], wo_s[w_rows, :])
    for d in (1, 2, 3):
        g_copies[d - 1].wait()
        w_rows = pl.ds(pl.multiple_of(((x + NX - d) % NX) * 256, 256), 256)
        proj = proj + dot(grecv[d], wo_s[w_rows, :])
    middle = (res_s[...].astype(F32) + proj).astype(BF)
    mid_s[...] = middle
    mid_w = middle.astype(F32)
    scale = lax.rsqrt(jnp.mean(mid_w * mid_w, axis=-1, keepdims=True) + EPS)
    normed = (mid_w * scale * egain_ref[...]).astype(BF)
    nrm_s[0:128, :] = normed[:, 0:1024]
    nrm_s[128:256, :] = normed[:, 1024:2048]

    def target(i, sign):
        k = (i * STRIDE) % DEVS
        return place(
            z + NZ + sign * (k // 32), y + NY + sign * ((k // 8) % 4),
            c + NC + sign * (k % 2), x + NX + sign * ((k // 2) % 4),
        )

    def send_copy(i):
        return pltpu.make_async_remote_copy(
            src_ref=send.at[i], dst_ref=recv.at[i],
            send_sem=ds.at[i // CHUNK], recv_sem=dr.at[i // CHUNK],
            device_id=target(i, 1), device_id_type=MESH,
        )

    def ret_copy(i):
        return pltpu.make_async_remote_copy(
            src_ref=ret.at[i], dst_ref=back.at[i],
            send_sem=es.at[i // CHUNK], recv_sem=er.at[i // CHUNK],
            device_id=target(i, -1), device_id_type=MESH,
        )

    def chunk_refs(first_slot, count, n, a, b, asem, bsem):
        return pltpu.make_async_remote_copy(
            src_ref=a.at[pl.ds(first_slot, count)], dst_ref=b.at[pl.ds(first_slot, count)],
            send_sem=asem.at[n], recv_sem=bsem.at[n],
            device_id=target(1, 1), device_id_type=MESH,
        )

    def start_range(make, lo, hi):
        def body(i, carry):
            make(i).start()
            return carry

        lax.fori_loop(lo, hi, body, 0)

    for n in range(8):
        rows = dot(lhs_s[256 * n : 256 * n + 256, :], nrm_s[...]).astype(BF).reshape(16, 16, 1024)
        send[16 * n : 16 * n + 16] = rows
        if n == 0:
            recv[0] = rows[0]
        start_range(send_copy, max(16 * n, 1), 16 * n + 16)

    l_cg.wait()
    l_cu.wait()
    l_cdn.wait()
    nrm = jnp.concatenate([nrm_s[0:128, :], nrm_s[128:256, :]], axis=1)
    hidden = (silu(dot(nrm, cg_s[...])) * dot(nrm, cu_s[...])).astype(BF)
    shared_s[...] = dot(hidden, cdn_s[...])

    l_wg.wait()
    l_wu.wait()
    l_wd.wait()
    pr = lax.broadcasted_iota(I32, (512, 512), 0)
    pc = lax.broadcasted_iota(I32, (512, 512), 1)
    want = ((pr >> 2) & 31) * 16 + ((pr >> 7) & 1) * 8 + (pr >> 8) * 4 + (pr & 3)
    pick = (pc == want).astype(F32).astype(BF)
    ur = lax.broadcasted_iota(I32, (256, 128), 0)
    uc = lax.broadcasted_iota(I32, (256, 128), 1)
    spread = [
        (((ur >> 3) == (uc >> 2)) & ((ur & 3) == (uc & 3)) & (((ur >> 2) & 1) == j))
        .astype(F32).astype(BF)
        for j in (0, 1)
    ]
    for n in range(CHUNKS):
        lo = 1 if n == 0 else 0
        chunk_refs(CHUNK * n + lo, CHUNK - lo, n, send, recv, ds, dr).wait_recv()
        block = recv[CHUNK * n : CHUNK * n + CHUNK].reshape(CHUNK * 16, 1024)
        picked = dot(pick, block).astype(BF)
        acts = []
        for j in (0, 1):
            rows = jnp.concatenate(
                [picked[256 * j : 256 * j + 128], picked[256 * j + 128 : 256 * j + 256]], axis=1
            )
            act = (silu(dot(rows, wg_s[j])) * dot(rows, wu_s[j])).astype(BF)
            acts.append(dot(spread[j], act).astype(BF))
        both = jnp.concatenate(acts, axis=1)
        done = dot(both, wd_s[...].reshape(1024, 2048))
        packed = jnp.concatenate(
            [done[:, 0:1024].reshape(CHUNK, 8, 1024), done[:, 1024:2048].reshape(CHUNK, 8, 1024)],
            axis=1,
        ).astype(BF)
        ret[CHUNK * n : CHUNK * n + CHUNK] = packed
        if n == 0:
            back[0] = packed[0]
        start_range(ret_copy, CHUNK * n + lo, CHUNK * n + CHUNK)

    for n in range(CHUNKS):
        lo = 1 if n == 0 else 0
        chunk_refs(CHUNK * n + lo, CHUNK - lo, n, ret, back, es, er).wait_recv()
        block = back[CHUNK * n : CHUNK * n + CHUNK].reshape(CHUNK * 16, 1024)
        part = dot(cw_s[:, 512 * n : 512 * n + 512], block)
        if n == 0:
            acc_s[...] = part
        else:
            acc_s[...] += part
    for h in (0, 1):
        cs = slice(1024 * h, 1024 * h + 1024)
        out_ref[:, cs] = (
            mid_s[:, cs].astype(F32) + acc_s[128 * h : 128 * h + 128, :] + shared_s[:, cs]
        ).astype(BF)
    for n in range(CHUNKS):
        lo = 1 if n == 0 else 0
        chunk_refs(CHUNK * n + lo, CHUNK - lo, n, send, recv, ds, dr).wait_send()
        chunk_refs(CHUNK * n + lo, CHUNK - lo, n, ret, back, es, er).wait_send()


def on_device(
    queries, key_matrix, value_matrix, channel_decay_input, head_decay_offset, output_gate_input,
    head_norm_gain, residual, mixer_output_weight, expert_norm_gain, routes, chosen_router_scores,
    routed_gate_weight, routed_up_weight, routed_down_weight, common_gate_weight,
    common_up_weight, common_down_weight,
):
    any_ = pl.BlockSpec(memory_space=pl.ANY)
    vm = pl.BlockSpec(memory_space=pltpu.VMEM)
    dma = pltpu.SemaphoreType.DMA
    V = pltpu.VMEM
    return pl.pallas_call(
        kernel,
        out_shape=jax.ShapeDtypeStruct((128, 2048), BF),
        in_specs=[
            any_, any_, any_, any_, vm, any_, vm, any_, any_, vm,
            vm, vm, any_, any_, any_, any_, any_, any_,
        ],
        out_specs=vm,
        scratch_shapes=[
            V((512, 128), BF), V((512, 128), BF), V((512, 256), BF), V((512, 128), BF),
            V((512, 256), BF), V((128, 2048), BF), V((1024, 2048), BF),
            V((2, 2048, 512), BF), V((2, 2048, 512), BF), V((2, 512, 2048), BF),
            V((2048, 512), BF), V((2048, 512), BF), V((512, 2048), BF),
            V((144, 128), BF), V((144, 128), BF), V((NY, 144, 128), BF), V((NZ, 144, 128), BF),
            V((2, 512, 128), F32), V((512, 128), BF), V((4, 128, 256), BF), V((4, 128, 256), BF),
            V((128, 2048), BF), V((256, 1024), BF), V((128, 2048), F32),
            V((2048, 256), BF), V((256, 2048), BF),
            V((DEVS, 16, 1024), BF), V((DEVS, 16, 1024), BF),
            V((DEVS, 16, 1024), BF), V((DEVS, 16, 1024), BF),
            V((256, 1024), F32),
            dma((13,)), dma, dma, dma((4,)), dma((4,)), dma((4,)), dma((4,)), dma((4,)), dma((4,)),
            dma((CHUNKS,)), dma((CHUNKS,)), dma((CHUNKS,)), dma((CHUNKS,)),
        ],
        compiler_params=pltpu.CompilerParams(
            collective_id=0, has_side_effects=True, vmem_limit_bytes=62 * 1024 * 1024
        ),
        name="layer",
    )(
        queries, key_matrix, value_matrix, channel_decay_input, head_decay_offset,
        output_gate_input, head_norm_gain.reshape(1, 128), residual, mixer_output_weight,
        expert_norm_gain.reshape(1, 2048), routes, chosen_router_scores, routed_gate_weight,
        routed_up_weight, routed_down_weight, common_gate_weight, common_up_weight,
        common_down_weight,
    )


def solution(mesh):
    both = ("sp", "tp")
    split, rows, rep = P("sp", "tp"), P(both, None), P()
    return jax.shard_map(
        on_device,
        mesh=mesh,
        in_specs=(
            split, split, split, split, split, split, rep, rows, rep, rep, rows, rows,
            P(both, None, None), P(both, None, None), P(both, None, None), rep, rep, rep,
        ),
        out_specs=rows,
        check_vma=False,
    )
```

```python
import jax
import jax.numpy as jnp
from jax import lax
from jax.experimental import pallas as pl
from jax.experimental.pallas import tpu as pltpu
from jax.sharding import PartitionSpec as P

MESH = pl.DeviceIdType.MESH
BF = jnp.bfloat16
F32 = jnp.float32
I32 = jnp.int32

BLOCK = 64
NZ, NY, NC, NX = 4, 4, 2, 4
DEVS = NZ * NY * NC * NX
STRIDE = 37
CHUNK = 32
CHUNKS = DEVS // CHUNK

EPS = 1e-6
RUNNING = 16.0
SCALE = 2.5


def dot(a, b):
    return jnp.dot(a, b, preferred_element_type=F32)


def dot_nt(a, b):
    return lax.dot_general(a, b, (((1,), (1,)), ((), ())), preferred_element_type=F32)


def dot_tn(a, b):
    return lax.dot_general(a, b, (((0,), (0,)), ((), ())), preferred_element_type=F32)


def silu(v):
    return v / (1.0 + jnp.exp(-v))


def three(v):
    hi = v.astype(BF)
    rest = v - hi.astype(F32)
    mid = rest.astype(BF)
    low = (rest - mid.astype(F32)).astype(BF)
    return hi, mid, low


def kernel(
    q_hbm, k_hbm, v_hbm, cd_hbm, hd_ref, og_hbm, hgain_ref, res_hbm, wo_hbm, egain_ref,
    routes_ref, scores_ref, wg_hbm, wu_hbm, wd_hbm, cg_hbm, cu_hbm, cdn_hbm,
    out_ref,
    q_s, k_s, v_s, cd_s, og_s, res_s, wo_s, wg_s, wu_s, wd_s, cg_s, cu_s, cdn_s,
    st1, st1r, st2, st3, outacc, qx_s, gsend, grecv, mid_s, nrm_s, shared_s,
    lhs_s, cw_s, send, recv, ret, back, acc_s,
    load_sem, s1, r1, s2, r2, s3, r3, gs, gr, ds, dr, es, er,
):
    sp = lax.axis_index("sp")
    x = lax.axis_index("tp")
    z = sp // (NY * NC)
    y = (sp // NC) % NY
    c = sp % NC

    def place(zz, yy, cc, xx):
        return ((zz % NZ) * (NY * NC) + (yy % NY) * NC + cc % NC, xx % NX)

    loads = [
        pltpu.make_async_copy(a, b, load_sem.at[n])
        for n, (a, b) in enumerate(
            (
                (cd_hbm, cd_s), (k_hbm, k_s), (v_hbm, v_s), (q_hbm, q_s), (og_hbm, og_s),
                (wo_hbm, wo_s), (res_hbm, res_s), (cg_hbm, cg_s), (cu_hbm, cu_s),
                (cdn_hbm, cdn_s), (wg_hbm, wg_s), (wu_hbm, wu_s), (wd_hbm, wd_s),
            )
        )
    ]
    for one in loads[:5]:
        one.start()
    (l_cd, l_k, l_v, l_q, l_og, l_wo, l_res, l_cg, l_cu, l_cdn, l_wg, l_wu, l_wd) = loads

    bar = pltpu.get_barrier_semaphore()
    neighbours = [place(z, y, c + 1, x)]
    neighbours += [place(z, y + d, c, x) for d in (1, 2, 3)]
    neighbours += [place(z + d, y, c, x) for d in (1, 2, 3)]
    neighbours += [place(z, y, c, x + d) for d in (1, 2, 3)]
    for one in neighbours:
        pl.semaphore_signal(bar, inc=1, device_id=one, device_id_type=MESH)

    lane = lax.broadcasted_iota(I32, (1, 128), 1)
    first = lane < 64
    rows_i = lax.broadcasted_iota(I32, (256, 256), 0)
    cols_i = lax.broadcasted_iota(I32, (256, 256), 1)
    causal = (rows_i >= cols_i) & ((rows_i >> 6) == (cols_i >> 6))
    tri = causal.astype(F32).astype(BF)
    hd_t = jnp.concatenate([hd_ref[...], jnp.zeros((6, 512), F32)], axis=0).T
    hd = jnp.where(first, hd_t[:, 0:1], hd_t[:, 1:2])
    l_cd.wait()
    cd = cd_s[...].astype(F32)
    dl = (jnp.minimum(cd, 0.0) - jnp.log1p(jnp.exp(-jnp.abs(cd)))) / RUNNING + hd
    parts = three(dl)
    within = jnp.concatenate(
        [sum(dot(tri, p[256 * n : 256 * n + 256]) for p in parts) for n in (0, 1)], axis=0
    )
    w3 = within.reshape(8, BLOCK, 128)
    ends = [w3[n, BLOCK - 1 : BLOCK, :] for n in range(8)]
    incl = []
    running = jnp.zeros((1, 128), F32)
    for n in range(8):
        running = running + ends[n]
        incl.append(running)
    total = incl[7]
    excl3 = jnp.stack([incl[n] - ends[n] for n in range(8)], axis=0)
    ends3 = jnp.stack(ends, axis=0)

    l_k.wait()
    l_v.wait()
    k = k_s[...].astype(F32)
    k3 = k.reshape(8, BLOCK, 128)
    k_tt = (k3 * jnp.exp(total[None] - excl3 - w3)).reshape(512, 128).astype(BF)
    v0, v1 = v_s[:, 0:128], v_s[:, 128:256]
    own_state = jnp.where(first, dot_tn(v0, k_tt), dot_tn(v1, k_tt))

    row16 = lax.broadcasted_iota(I32, (16, 128), 0)

    def put_state(ref, log, state):
        ref[0:128, :] = state.astype(BF)
        hi, mid, low = (p.astype(F32) for p in three(log))
        tail = jnp.where(row16 == 0, hi, jnp.where(row16 == 1, mid, jnp.where(row16 == 2, low, 0.0)))
        ref[128:144, :] = tail.astype(BF)

    def get_state(ref):
        log = jnp.sum(ref[128:144, :].astype(F32), axis=0, keepdims=True)
        return log, ref[0:128, :].astype(F32)

    put_state(st1, total, own_state)
    pl.semaphore_wait(bar, 10)
    core_copy = pltpu.make_async_remote_copy(
        src_ref=st1, dst_ref=st1r, send_sem=s1, recv_sem=r1,
        device_id=place(z, y, c + 1, x), device_id_type=MESH,
    )
    core_copy.start()
    for one in loads[5:]:
        one.start()

    l_q.wait()
    ew = jnp.exp(within)
    qd = q_s[...].astype(F32) * 0.125 * ew
    qx_s[...] = (qd.reshape(8, BLOCK, 128) * jnp.exp(excl3)).reshape(512, 128).astype(BF)
    kg = (k * jnp.exp(-within)).astype(BF)
    for h in (0, 1):
        q_h = jnp.where(first if h == 0 else ~first, qd, 0.0).astype(BF)
        v_h = v0 if h == 0 else v1
        for n in (0, 1):
            sl = slice(256 * n, 256 * n + 256)
            scores = jnp.where(causal, dot_nt(q_h[sl], kg[sl]), 0.0).astype(BF)
            outacc[h, sl, :] = dot(scores, v_h[sl])

    core_copy.wait()
    core1 = c == 1
    log_p, state_p = get_state(st1r)
    pair_log = total + log_p
    pair_state = jnp.where(
        core1,
        jnp.exp(total) * state_p + own_state,
        jnp.exp(log_p) * own_state + state_p,
    )
    carry_log = jnp.where(core1, log_p, 0.0)
    carry_state = jnp.where(core1, state_p, 0.0)

    def exchange(slots, mine, log, state, ssem, rsem, target):
        put_state(slots.at[mine], log, state)
        copies = []
        for d in (1, 2, 3):
            one = pltpu.make_async_remote_copy(
                src_ref=slots.at[mine], dst_ref=slots.at[mine],
                send_sem=ssem.at[d], recv_sem=rsem.at[d],
                device_id=target(d), device_id_type=MESH,
            )
            one.start()
            copies.append(one)
        return copies

    def prefix(slots, mine, count, carry_log, carry_state):
        run_log = jnp.zeros((1, 128), F32)
        run_state = jnp.zeros((128, 128), F32)
        pre_log, pre_state = run_log, run_state
        for n in range(count):
            pre_log = jnp.where(mine == n, run_log, pre_log)
            pre_state = jnp.where(mine == n, run_state, pre_state)
            log, state = get_state(slots.at[n])
            run_state = jnp.exp(log) * run_state + state
            run_log = run_log + log
        carry_state = jnp.exp(carry_log) * pre_state + carry_state
        carry_log = carry_log + pre_log
        return run_log, run_state, carry_log, carry_state

    y_copies = exchange(st2, y, pair_log, pair_state, s2, r2, lambda d: place(z, y + d, c, x))

    k_tail = (k3 * jnp.exp(ends3 - w3)).reshape(512, 128).astype(BF)
    state = jnp.zeros((128, 128), F32)
    for n in range(8):
        sl = slice(BLOCK * n, BLOCK * n + BLOCK)
        if n > 0:
            state_b = state.astype(BF)
            for h in (0, 1):
                q_h = jnp.where(first if h == 0 else ~first, qd[sl], 0.0).astype(BF)
                outacc[h, sl, :] += dot_nt(q_h, state_b)
        if n < 7:
            added = jnp.where(first, dot_tn(v0[sl], k_tail[sl]), dot_tn(v1[sl], k_tail[sl]))
            state = jnp.exp(ends[n]) * state + added

    for one in y_copies:
        one.wait()
    plane_log, plane_state, carry_log, carry_state = prefix(st2, y, NY, carry_log, carry_state)
    z_copies = exchange(st3, z, plane_log, plane_state, s3, r3, lambda d: place(z + d, y, c, x))

    def expert_of(index):
        off = ((index >> 4) * STRIDE) & (DEVS - 1)
        dev = ((z + (off >> 5)) & 3) * 8 + ((y + (off >> 3)) & 3) * 2 + ((c + off) & 1)
        return (dev * 4 + ((x + (off >> 1)) & 3)) * 2 + ((index >> 2) & 1)

    turned = routes_ref[...].astype(F32)
    routes = jnp.concatenate([turned, jnp.zeros((124, 128), F32)], axis=0).T
    sub128 = lax.broadcasted_iota(I32, (128, 128), 0)
    lan128 = lax.broadcasted_iota(I32, (128, 128), 1)
    upper = (sub128 < lan128).astype(F32).astype(BF)
    lower = (sub128 > lan128).astype(F32).astype(BF)
    for n in range(8):
        q_index = lax.broadcasted_iota(I32, (256, 128), 0) + 256 * n
        expert = expert_of(q_index).astype(F32)
        match = jnp.zeros((256, 128), F32)
        for j in range(4):
            match = jnp.where(expert == turned[j : j + 1, :], 1.0, match)
        rank = dot(match.astype(BF), upper)
        live = jnp.where(rank == (q_index & 3).astype(F32), match, 0.0)
        half = ((q_index >> 3) & 1) == 0
        lhs_s[256 * n : 256 * n + 256, 0:128] = jnp.where(half, live, 0.0).astype(BF)
        lhs_s[256 * n : 256 * n + 256, 128:256] = jnp.where(half, 0.0, live).astype(BF)
    scores = scores_ref[...]
    weights = SCALE * scores / jnp.sum(scores, axis=0, keepdims=True)
    weights = jnp.concatenate([weights, jnp.zeros((124, 128), F32)], axis=0).T
    for n in range(4):
        q_index = lax.broadcasted_iota(I32, (128, 512), 1) + 512 * n
        expert = expert_of(q_index).astype(F32)
        weight = jnp.zeros((128, 512), F32)
        match = jnp.zeros((128, 512), F32)
        for j in range(4):
            hit = expert == routes[:, j : j + 1]
            match = jnp.where(hit, 1.0, match)
            weight = jnp.where(hit, weights[:, j : j + 1], weight)
        rank = dot(lower, match.astype(BF))
        weight = jnp.where(rank == (q_index & 3).astype(F32), weight, 0.0)
        half = ((q_index >> 3) & 1) == 0
        cw_s[0:128, 512 * n : 512 * n + 512] = jnp.where(half, weight, 0.0).astype(BF)
        cw_s[128:256, 512 * n : 512 * n + 512] = jnp.where(half, 0.0, weight).astype(BF)

    for one in z_copies:
        one.wait()
    _, _, _, carried = prefix(st3, z, NZ, carry_log, carry_state)
    carried_b = carried.astype(BF)

    l_og.wait()
    g_copies = []
    for d in (1, 2, 3, 0):
        xx = (x + d) % NX
        rows = pl.ds(pl.multiple_of(xx * 128, 128), 128)
        qx = qx_s[rows, :]
        for h in (0, 1):
            q_h = jnp.where(first if h == 0 else ~first, qx.astype(F32), 0.0).astype(BF)
            attn = outacc[h, rows, :] + dot_nt(q_h, carried_b)
            inv = lax.rsqrt(jnp.mean(attn * attn, axis=-1, keepdims=True) + EPS)
            gate = og_s[rows, 128 * h : 128 * h + 128].astype(F32)
            value = attn * inv * hgain_ref[...] * silu(gate)
            gsend[d, :, 128 * h : 128 * h + 128] = value.astype(BF)
        if d > 0:
            one = pltpu.make_async_remote_copy(
                src_ref=gsend.at[d], dst_ref=grecv.at[d], send_sem=gs.at[d], recv_sem=gr.at[d],
                device_id=place(z, y, c, x + d), device_id_type=MESH,
            )
            one.start()
            g_copies.append(one)

    l_wo.wait()
    l_res.wait()
    w_rows = pl.ds(pl.multiple_of(x * 256, 256), 256)
    proj = dot(gsend[0], wo_s[w_rows, :])
    for d in (1, 2, 3):
        g_copies[d - 1].wait()
        w_rows = pl.ds(pl.multiple_of(((x + NX - d) % NX) * 256, 256), 256)
        proj = proj + dot(grecv[d], wo_s[w_rows, :])
    middle = (res_s[...].astype(F32) + proj).astype(BF)
    mid_s[...] = middle
    mid_w = middle.astype(F32)
    scale = lax.rsqrt(jnp.mean(mid_w * mid_w, axis=-1, keepdims=True) + EPS)
    normed = (mid_w * scale * egain_ref[...]).astype(BF)
    nrm_s[0:128, :] = normed[:, 0:1024]
    nrm_s[128:256, :] = normed[:, 1024:2048]

    def target(i, sign):
        k = (i * STRIDE) % DEVS
        return place(
            z + NZ + sign * (k // 32), y + NY + sign * ((k // 8) % 4),
            c + NC + sign * (k % 2), x + NX + sign * ((k // 2) % 4),
        )

    def send_copy(i):
        return pltpu.make_async_remote_copy(
            src_ref=send.at[i], dst_ref=recv.at[i],
            send_sem=ds.at[i // CHUNK], recv_sem=dr.at[i // CHUNK],
            device_id=target(i, 1), device_id_type=MESH,
        )

    def ret_copy(i):
        return pltpu.make_async_remote_copy(
            src_ref=ret.at[i], dst_ref=back.at[i],
            send_sem=es.at[i // CHUNK], recv_sem=er.at[i // CHUNK],
            device_id=target(i, -1), device_id_type=MESH,
        )

    def chunk_refs(first_slot, count, n, a, b, asem, bsem):
        return pltpu.make_async_remote_copy(
            src_ref=a.at[pl.ds(first_slot, count)], dst_ref=b.at[pl.ds(first_slot, count)],
            send_sem=asem.at[n], recv_sem=bsem.at[n],
            device_id=target(1, 1), device_id_type=MESH,
        )

    def start_range(make, lo, hi):
        def body(i, carry):
            make(i).start()
            return carry

        lax.fori_loop(lo, hi, body, 0)

    for n in range(8):
        rows = dot(lhs_s[256 * n : 256 * n + 256, :], nrm_s[...]).astype(BF).reshape(16, 16, 1024)
        send[16 * n : 16 * n + 16] = rows
        if n == 0:
            recv[0] = rows[0]
        start_range(send_copy, max(16 * n, 1), 16 * n + 16)

    l_cg.wait()
    l_cu.wait()
    l_cdn.wait()
    nrm = jnp.concatenate([nrm_s[0:128, :], nrm_s[128:256, :]], axis=1)
    hidden = (silu(dot(nrm, cg_s[...])) * dot(nrm, cu_s[...])).astype(BF)
    shared_s[...] = dot(hidden, cdn_s[...])

    l_wg.wait()
    l_wu.wait()
    l_wd.wait()
    pr = lax.broadcasted_iota(I32, (512, 512), 0)
    pc = lax.broadcasted_iota(I32, (512, 512), 1)
    want = ((pr >> 2) & 31) * 16 + ((pr >> 7) & 1) * 8 + (pr >> 8) * 4 + (pr & 3)
    pick = (pc == want).astype(F32).astype(BF)
    ur = lax.broadcasted_iota(I32, (256, 128), 0)
    uc = lax.broadcasted_iota(I32, (256, 128), 1)
    spread = [
        (((ur >> 3) == (uc >> 2)) & ((ur & 3) == (uc & 3)) & (((ur >> 2) & 1) == j))
        .astype(F32).astype(BF)
        for j in (0, 1)
    ]
    for n in range(CHUNKS):
        lo = 1 if n == 0 else 0
        chunk_refs(CHUNK * n + lo, CHUNK - lo, n, send, recv, ds, dr).wait_recv()
        block = recv[CHUNK * n : CHUNK * n + CHUNK].reshape(CHUNK * 16, 1024)
        picked = dot(pick, block).astype(BF)
        acts = []
        for j in (0, 1):
            rows = jnp.concatenate(
                [picked[256 * j : 256 * j + 128], picked[256 * j + 128 : 256 * j + 256]], axis=1
            )
            act = (silu(dot(rows, wg_s[j])) * dot(rows, wu_s[j])).astype(BF)
            acts.append(dot(spread[j], act).astype(BF))
        both = jnp.concatenate(acts, axis=1)
        done = dot(both, wd_s[...].reshape(1024, 2048))
        packed = jnp.concatenate(
            [done[:, 0:1024].reshape(CHUNK, 8, 1024), done[:, 1024:2048].reshape(CHUNK, 8, 1024)],
            axis=1,
        ).astype(BF)
        ret[CHUNK * n : CHUNK * n + CHUNK] = packed
        if n == 0:
            back[0] = packed[0]
        start_range(ret_copy, CHUNK * n + lo, CHUNK * n + CHUNK)

    for n in range(CHUNKS):
        lo = 1 if n == 0 else 0
        chunk_refs(CHUNK * n + lo, CHUNK - lo, n, ret, back, es, er).wait_recv()
        block = back[CHUNK * n : CHUNK * n + CHUNK].reshape(CHUNK * 16, 1024)
        part = dot(cw_s[:, 512 * n : 512 * n + 512], block)
        if n == 0:
            acc_s[...] = part
        else:
            acc_s[...] += part
    for h in (0, 1):
        cs = slice(1024 * h, 1024 * h + 1024)
        out_ref[:, cs] = (
            mid_s[:, cs].astype(F32) + acc_s[128 * h : 128 * h + 128, :] + shared_s[:, cs]
        ).astype(BF)
    for n in range(CHUNKS):
        lo = 1 if n == 0 else 0
        chunk_refs(CHUNK * n + lo, CHUNK - lo, n, send, recv, ds, dr).wait_send()
        chunk_refs(CHUNK * n + lo, CHUNK - lo, n, ret, back, es, er).wait_send()


def on_device(
    queries, key_matrix, value_matrix, channel_decay_input, head_decay_offset, output_gate_input,
    head_norm_gain, residual, mixer_output_weight, expert_norm_gain, routes, chosen_router_scores,
    routed_gate_weight, routed_up_weight, routed_down_weight, common_gate_weight,
    common_up_weight, common_down_weight,
):
    any_ = pl.BlockSpec(memory_space=pl.ANY)
    vm = pl.BlockSpec(memory_space=pltpu.VMEM)
    dma = pltpu.SemaphoreType.DMA
    V = pltpu.VMEM
    return pl.pallas_call(
        kernel,
        out_shape=jax.ShapeDtypeStruct((128, 2048), BF),
        in_specs=[
            any_, any_, any_, any_, vm, any_, vm, any_, any_, vm,
            vm, vm, any_, any_, any_, any_, any_, any_,
        ],
        out_specs=vm,
        scratch_shapes=[
            V((512, 128), BF), V((512, 128), BF), V((512, 256), BF), V((512, 128), BF),
            V((512, 256), BF), V((128, 2048), BF), V((1024, 2048), BF),
            V((2, 2048, 512), BF), V((2, 2048, 512), BF), V((2, 512, 2048), BF),
            V((2048, 512), BF), V((2048, 512), BF), V((512, 2048), BF),
            V((144, 128), BF), V((144, 128), BF), V((NY, 144, 128), BF), V((NZ, 144, 128), BF),
            V((2, 512, 128), F32), V((512, 128), BF), V((4, 128, 256), BF), V((4, 128, 256), BF),
            V((128, 2048), BF), V((256, 1024), BF), V((128, 2048), F32),
            V((2048, 256), BF), V((256, 2048), BF),
            V((DEVS, 16, 1024), BF), V((DEVS, 16, 1024), BF),
            V((DEVS, 16, 1024), BF), V((DEVS, 16, 1024), BF),
            V((256, 1024), F32),
            dma((13,)), dma, dma, dma((4,)), dma((4,)), dma((4,)), dma((4,)), dma((4,)), dma((4,)),
            dma((CHUNKS,)), dma((CHUNKS,)), dma((CHUNKS,)), dma((CHUNKS,)),
        ],
        compiler_params=pltpu.CompilerParams(
            collective_id=0, has_side_effects=True, vmem_limit_bytes=62 * 1024 * 1024
        ),
        name="layer",
    )(
        queries, key_matrix, value_matrix, channel_decay_input, head_decay_offset.T,
        output_gate_input, head_norm_gain.reshape(1, 128), residual, mixer_output_weight,
        expert_norm_gain.reshape(1, 2048), routes.T, chosen_router_scores.T, routed_gate_weight,
        routed_up_weight, routed_down_weight, common_gate_weight, common_up_weight,
        common_down_weight,
    )


def solution(mesh):
    both = ("sp", "tp")
    split, rows, rep = P("sp", "tp"), P(both, None), P()
    return jax.shard_map(
        on_device,
        mesh=mesh,
        in_specs=(
            split, split, split, split, split, split, rep, rows, rep, rep, rows, rows,
            P(both, None, None), P(both, None, None), P(both, None, None), rep, rep, rep,
        ),
        out_specs=rows,
        check_vma=False,
    )
```

```python
import jax
import jax.numpy as jnp
from jax import lax
from jax.experimental import pallas as pl
from jax.experimental.pallas import tpu as pltpu
from jax.sharding import PartitionSpec as P

MESH = pl.DeviceIdType.MESH
BF = jnp.bfloat16
F32 = jnp.float32
I32 = jnp.int32

BLOCK = 64
NZ, NY, NC, NX = 4, 4, 2, 4
DEVS = NZ * NY * NC * NX
STEP = 5
WIDTHS = (640, 640, 768)
STARTS = (0, 640, 1280)
AXES = (0, 1, 2)

EPS = 1e-6
RUNNING = 16.0
SCALE = 2.5


def dot(a, b):
    return jnp.dot(a, b, preferred_element_type=F32)


def dot_nt(a, b):
    return lax.dot_general(a, b, (((1,), (1,)), ((), ())), preferred_element_type=F32)


def dot_tn(a, b):
    return lax.dot_general(a, b, (((0,), (0,)), ((), ())), preferred_element_type=F32)


def silu(v):
    return v / (1.0 + jnp.exp(-v))


def three(v):
    hi = v.astype(BF)
    rest = v - hi.astype(F32)
    mid = rest.astype(BF)
    low = (rest - mid.astype(F32)).astype(BF)
    return hi, mid, low


def kernel(
    q_hbm, k_hbm, v_hbm, cd_hbm, hd_ref, og_hbm, hgain_ref, res_hbm, wo_hbm, egain_ref,
    routes_ref, scores_ref, wg_hbm, wu_hbm, wd_hbm, cg_hbm, cu_hbm, cdn_hbm,
    out_ref,
    q_s, k_s, v_s, cd_s, og_s, res_s, wo_s, wg_s, wu_s, wd_s, cg_s, cu_s, cdn_s,
    st1, st1r, st2, st3, outacc, qx_s, gsend, grecv, mid_s, shared_s,
    rt_s, lhs_s, cw_s, pick_s, place_s,
    bx, by, bz, px, py, pz, sx, sy, sz, rx, ry, rz, tx, ty, tz, kx, ky, kz,
    load_sem, s1, r1, s2, r2, s3, r3, gs, gr,
    ts, tr, bs, br, ds, dr, es, er, ps, pr,
):
    sp = lax.axis_index("sp")
    x = lax.axis_index("tp")
    z = sp // (NY * NC)
    y = (sp // NC) % NY
    c = sp % NC

    def place(zz, yy, cc, xx):
        return ((zz % NZ) * (NY * NC) + (yy % NY) * NC + cc % NC, xx % NX)

    lines, sums = (bx, by, bz), (px, py, pz)
    send, recv, ret, back = (sx, sy, sz), (rx, ry, rz), (tx, ty, tz), (kx, ky, kz)

    def along(a, d):
        return place(z + (d if a == 2 else 0), y + (d if a == 1 else 0), c, x + (d if a == 0 else 0))

    def across(a, n, i, sign):
        k = (i * STEP) % 16
        d1, d2, dc = sign * (k // 4), sign * (k % 4), sign * n
        if a == 0:
            return place(z + NZ + d1, y + NY + d2, c + NC + dc, x)
        if a == 1:
            return place(z + NZ + d1, y, c + NC + dc, x + NX + d2)
        return place(z, y + NY + d1, c + NC + dc, x + NX + d2)

    def plane_split(i):
        k = (i * STEP) & 15
        return k >> 2, k & 3

    def expert_of(a, n, i, j):
        d1, d2 = plane_split(i)
        zz = (z + (0 if a == 2 else d1)) & 3
        yy = (y + (0 if a == 1 else (d2 if a == 0 else d1))) & 3
        xx = (x + (0 if a == 0 else d2)) & 3
        return ((zz * 8 + yy * 2 + ((c + n) & 1)) * 4 + xx) * 2 + j

    def line_copy(a, d, src, dst, ssem, rsem, sign):
        return pltpu.make_async_remote_copy(
            src_ref=src, dst_ref=dst, send_sem=ssem.at[4 * a + d], recv_sem=rsem.at[4 * a + d],
            device_id=along(a, d if sign > 0 else 4 - d), device_id_type=MESH,
        )

    loads = [
        pltpu.make_async_copy(a, b, load_sem.at[n])
        for n, (a, b) in enumerate(
            (
                (cd_hbm, cd_s), (k_hbm, k_s), (v_hbm, v_s), (q_hbm, q_s), (og_hbm, og_s),
                (wo_hbm, wo_s), (res_hbm, res_s), (cg_hbm, cg_s), (cu_hbm, cu_s),
                (cdn_hbm, cdn_s), (wg_hbm, wg_s), (wu_hbm, wu_s), (wd_hbm, wd_s),
            )
        )
    ]
    for one in loads[:5]:
        one.start()
    (l_cd, l_k, l_v, l_q, l_og, l_wo, l_res, l_cg, l_cu, l_cdn, l_wg, l_wu, l_wd) = loads

    bar = pltpu.get_barrier_semaphore()
    neighbours = [place(z, y, c + 1, x)]
    neighbours += [place(z, y + d, c, x) for d in (1, 2, 3)]
    neighbours += [place(z + d, y, c, x) for d in (1, 2, 3)]
    neighbours += [place(z, y, c, x + d) for d in (1, 2, 3)]
    for one in neighbours:
        pl.semaphore_signal(bar, inc=1, device_id=one, device_id_type=MESH)

    lane = lax.broadcasted_iota(I32, (1, 128), 1)
    first = lane < 64
    rows_i = lax.broadcasted_iota(I32, (256, 256), 0)
    cols_i = lax.broadcasted_iota(I32, (256, 256), 1)
    causal = (rows_i >= cols_i) & ((rows_i >> 6) == (cols_i >> 6))
    tri = causal.astype(F32).astype(BF)
    hd_t = jnp.concatenate([hd_ref[...], jnp.zeros((6, 512), F32)], axis=0).T
    hd = jnp.where(first, hd_t[:, 0:1], hd_t[:, 1:2])
    l_cd.wait()
    cd = cd_s[...].astype(F32)
    dl = (jnp.minimum(cd, 0.0) - jnp.log1p(jnp.exp(-jnp.abs(cd)))) / RUNNING + hd
    parts = three(dl)
    within = jnp.concatenate(
        [sum(dot(tri, p[256 * n : 256 * n + 256]) for p in parts) for n in (0, 1)], axis=0
    )
    w3 = within.reshape(8, BLOCK, 128)
    ends = [w3[n, BLOCK - 1 : BLOCK, :] for n in range(8)]
    incl = []
    running = jnp.zeros((1, 128), F32)
    for n in range(8):
        running = running + ends[n]
        incl.append(running)
    total = incl[7]
    excl3 = jnp.stack([incl[n] - ends[n] for n in range(8)], axis=0)
    ends3 = jnp.stack(ends, axis=0)

    l_k.wait()
    l_v.wait()
    k = k_s[...].astype(F32)
    k3 = k.reshape(8, BLOCK, 128)
    k_tt = (k3 * jnp.exp(total[None] - excl3 - w3)).reshape(512, 128).astype(BF)
    v0, v1 = v_s[:, 0:128], v_s[:, 128:256]
    own_state = jnp.where(first, dot_tn(v0, k_tt), dot_tn(v1, k_tt))

    row16 = lax.broadcasted_iota(I32, (16, 128), 0)

    def put_state(ref, log, state):
        ref[0:128, :] = state.astype(BF)
        hi, mid, low = (p.astype(F32) for p in three(log))
        tail = jnp.where(row16 == 0, hi, jnp.where(row16 == 1, mid, jnp.where(row16 == 2, low, 0.0)))
        ref[128:144, :] = tail.astype(BF)

    def get_state(ref):
        log = jnp.sum(ref[128:144, :].astype(F32), axis=0, keepdims=True)
        return log, ref[0:128, :].astype(F32)

    put_state(st1, total, own_state)
    scores = scores_ref[...]
    weights = SCALE * scores / jnp.sum(scores, axis=0, keepdims=True)
    rt_s[0] = jnp.concatenate([routes_ref[...].astype(F32), weights], axis=0)
    pl.semaphore_wait(bar, 10)
    core_copy = pltpu.make_async_remote_copy(
        src_ref=st1, dst_ref=st1r, send_sem=s1, recv_sem=r1,
        device_id=place(z, y, c + 1, x), device_id_type=MESH,
    )
    core_copy.start()
    rt_copies = [
        line_copy(a, d, rt_s.at[0], rt_s.at[4 * a + d], ts, tr, 1) for a in AXES for d in (1, 2, 3)
    ]
    for one in rt_copies:
        one.start()
    for one in loads[5:]:
        one.start()

    l_q.wait()
    ew = jnp.exp(within)
    qd = q_s[...].astype(F32) * 0.125 * ew
    qx_s[...] = (qd.reshape(8, BLOCK, 128) * jnp.exp(excl3)).reshape(512, 128).astype(BF)
    kg = (k * jnp.exp(-within)).astype(BF)
    for h in (0, 1):
        q_h = jnp.where(first if h == 0 else ~first, qd, 0.0).astype(BF)
        v_h = v0 if h == 0 else v1
        for n in (0, 1):
            sl = slice(256 * n, 256 * n + 256)
            scores = jnp.where(causal, dot_nt(q_h[sl], kg[sl]), 0.0).astype(BF)
            outacc[h, sl, :] = dot(scores, v_h[sl])

    core_copy.wait()
    core1 = c == 1
    log_p, state_p = get_state(st1r)
    pair_log = total + log_p
    pair_state = jnp.where(
        core1,
        jnp.exp(total) * state_p + own_state,
        jnp.exp(log_p) * own_state + state_p,
    )
    carry_log = jnp.where(core1, log_p, 0.0)
    carry_state = jnp.where(core1, state_p, 0.0)

    def exchange(slots, mine, log, state, ssem, rsem, target):
        put_state(slots.at[mine], log, state)
        copies = []
        for d in (1, 2, 3):
            one = pltpu.make_async_remote_copy(
                src_ref=slots.at[mine], dst_ref=slots.at[mine],
                send_sem=ssem.at[d], recv_sem=rsem.at[d],
                device_id=target(d), device_id_type=MESH,
            )
            one.start()
            copies.append(one)
        return copies

    def prefix(slots, mine, count, carry_log, carry_state):
        run_log = jnp.zeros((1, 128), F32)
        run_state = jnp.zeros((128, 128), F32)
        pre_log, pre_state = run_log, run_state
        for n in range(count):
            pre_log = jnp.where(mine == n, run_log, pre_log)
            pre_state = jnp.where(mine == n, run_state, pre_state)
            log, state = get_state(slots.at[n])
            run_state = jnp.exp(log) * run_state + state
            run_log = run_log + log
        carry_state = jnp.exp(carry_log) * pre_state + carry_state
        carry_log = carry_log + pre_log
        return run_log, run_state, carry_log, carry_state

    y_copies = exchange(st2, y, pair_log, pair_state, s2, r2, lambda d: place(z, y + d, c, x))

    k_tail = (k3 * jnp.exp(ends3 - w3)).reshape(512, 128).astype(BF)
    state = jnp.zeros((128, 128), F32)
    for n in range(8):
        sl = slice(BLOCK * n, BLOCK * n + BLOCK)
        if n > 0:
            state_b = state.astype(BF)
            for h in (0, 1):
                q_h = jnp.where(first if h == 0 else ~first, qd[sl], 0.0).astype(BF)
                outacc[h, sl, :] += dot_nt(q_h, state_b)
        if n < 7:
            added = jnp.where(first, dot_tn(v0[sl], k_tail[sl]), dot_tn(v1[sl], k_tail[sl]))
            state = jnp.exp(ends[n]) * state + added

    for one in y_copies:
        one.wait()
    plane_log, plane_state, carry_log, carry_state = prefix(st2, y, NY, carry_log, carry_state)
    z_copies = exchange(st3, z, plane_log, plane_state, s3, r3, lambda d: place(z + d, y, c, x))

    for one in rt_copies:
        one.wait()
    sub128 = lax.broadcasted_iota(I32, (128, 128), 0)
    lan128 = lax.broadcasted_iota(I32, (128, 128), 1)
    upper = (sub128 < lan128).astype(F32).astype(BF)
    lower = (sub128 > lan128).astype(F32).astype(BF)
    nothing = jnp.zeros((32, 8, 128), F32)
    q_index = lax.broadcasted_iota(I32, (256, 128), 0)
    for a in AXES:
        expert = expert_of(a, q_index >> 7, (q_index >> 3) & 15, (q_index >> 2) & 1).astype(F32)
        for d in range(4):
            info = rt_s[4 * a + d if d else 0]
            match = jnp.zeros((256, 128), F32)
            for j in range(4):
                match = jnp.where(expert == info[j : j + 1, :], 1.0, match)
            rank = dot(match.astype(BF), upper)
            live = jnp.where(rank == (q_index & 3).astype(F32), match, 0.0).reshape(32, 8, 128)
            pair = [live, nothing] if d % 2 == 0 else [nothing, live]
            cols = slice(128 * (d % 2), 128 * (d % 2) + 128)
            lhs_s[2 * a + d // 2, :, cols] = (
                jnp.concatenate(pair, axis=1).reshape(512, 128).astype(BF)
            )

    for one in z_copies:
        one.wait()
    _, _, _, carried = prefix(st3, z, NZ, carry_log, carry_state)
    carried_b = carried.astype(BF)

    l_og.wait()
    g_copies = []
    for d in (1, 2, 3, 0):
        xx = (x + d) % NX
        rows = pl.ds(pl.multiple_of(xx * 128, 128), 128)
        qx = qx_s[rows, :]
        for h in (0, 1):
            q_h = jnp.where(first if h == 0 else ~first, qx.astype(F32), 0.0).astype(BF)
            attn = outacc[h, rows, :] + dot_nt(q_h, carried_b)
            inv = lax.rsqrt(jnp.mean(attn * attn, axis=-1, keepdims=True) + EPS)
            gate = og_s[rows, 128 * h : 128 * h + 128].astype(F32)
            value = attn * inv * hgain_ref[...] * silu(gate)
            gsend[d, :, 128 * h : 128 * h + 128] = value.astype(BF)
        if d > 0:
            one = pltpu.make_async_remote_copy(
                src_ref=gsend.at[d], dst_ref=grecv.at[d], send_sem=gs.at[d], recv_sem=gr.at[d],
                device_id=place(z, y, c, x + d), device_id_type=MESH,
            )
            one.start()
            g_copies.append(one)

    l_wo.wait()
    l_res.wait()
    w_rows = pl.ds(pl.multiple_of(x * 256, 256), 256)
    proj = dot(gsend[0], wo_s[w_rows, :])
    for d in (1, 2, 3):
        g_copies[d - 1].wait()
        w_rows = pl.ds(pl.multiple_of(((x + NX - d) % NX) * 256, 256), 256)
        proj = proj + dot(grecv[d], wo_s[w_rows, :])
    middle = (res_s[...].astype(F32) + proj).astype(BF)
    mid_s[...] = middle
    mid_w = middle.astype(F32)
    scale = lax.rsqrt(jnp.mean(mid_w * mid_w, axis=-1, keepdims=True) + EPS)
    normed = (mid_w * scale * egain_ref[...]).astype(BF)
    b_copies = {}
    for a in AXES:
        lines[a][0] = normed[:, STARTS[a] : STARTS[a] + WIDTHS[a]]
        for d in (1, 2, 3):
            b_copies[a, d] = line_copy(a, d, lines[a].at[0], lines[a].at[d], bs, br, 1)
    for d in (1, 3, 2):
        for a in AXES:
            b_copies[a, d].start()

    def sem(a, half, n):
        return 4 * a + 2 * half + n

    def plane_copies(half, n, source, dest, ssem, rsem, sign):
        def body(i, carry):
            for a in AXES:
                pltpu.make_async_remote_copy(
                    src_ref=source[a].at[n, half, i], dst_ref=dest[a].at[n, half, i],
                    send_sem=ssem.at[sem(a, half, n)], recv_sem=rsem.at[sem(a, half, n)],
                    device_id=across(a, n, i, sign), device_id_type=MESH,
                ).start()
            return carry

        lax.fori_loop(1 if n == 0 else 0, 16, body, 0)

    def plane_wait(a, half, n, source, dest, ssem, rsem):
        part = pl.ds(1, 15) if n == 0 else pl.ds(0, 16)
        return pltpu.make_async_remote_copy(
            src_ref=source[a].at[n, half, part], dst_ref=dest[a].at[n, half, part],
            send_sem=ssem.at[sem(a, half, n)], recv_sem=rsem.at[sem(a, half, n)],
            device_id=across(a, 1, 1, 1), device_id_type=MESH,
        )

    for n in (0, 1):
        for half in (0, 1):
            for a in AXES:
                if n == 0:
                    for d in (1,) if half == 0 else (3, 2):
                        b_copies[a, d].wait_recv()
                rows = dot(
                    lhs_s[2 * a + half, 256 * n : 256 * n + 256, :],
                    lines[a][2 * half : 2 * half + 2].reshape(256, WIDTHS[a]),
                ).astype(BF).reshape(16, 16, WIDTHS[a])
                send[a][n, half] = rows
                if n == 0:
                    recv[a][0, half, 0] = rows[0]
            plane_copies(half, n, send, recv, ds, dr, 1)

    l_cg.wait()
    l_cu.wait()
    l_cdn.wait()
    nrm = jnp.concatenate([lines[a][0] for a in AXES], axis=1)
    hidden = (silu(dot(nrm, cg_s[...])) * dot(nrm, cu_s[...])).astype(BF)
    shared_s[...] = dot(hidden, cdn_s[...])

    def row_of(a, q):
        d1, d2 = plane_split((q >> 4) & 15)
        d = ((q >> 8) & 1) * 2 + ((q >> 3) & 1)
        dz, dy, dx = ((d1, d2, d), (d1, d, d2), (d, d1, d2))[a]
        return ((q >> 2) & 1) * 256 + (dz * 16 + dy * 4 + dx) * 4 + (q & 3)

    down = lax.broadcasted_iota(I32, (512, 512), 0)
    over = lax.broadcasted_iota(I32, (512, 512), 1)
    for a in AXES:
        pick_s[a] = (down == row_of(a, over)).astype(F32).astype(BF)
        place_s[a] = (over == row_of(a, down)).astype(F32).astype(BF)
    q_index = lax.broadcasted_iota(I32, (128, 512), 1)
    blank = jnp.zeros((120, 128), F32)
    for a in AXES:
        expert = expert_of(a, q_index >> 8, (q_index >> 4) & 15, (q_index >> 2) & 1).astype(F32)
        for d in range(4):
            info = jnp.concatenate([rt_s[4 * a + d if d else 0], blank], axis=0).T
            weight = jnp.zeros((128, 512), F32)
            match = jnp.zeros((128, 512), F32)
            for j in range(4):
                hit = expert == info[:, j : j + 1]
                match = jnp.where(hit, 1.0, match)
                weight = jnp.where(hit, info[:, 4 + j : 5 + j], weight)
            rank = dot(lower, match.astype(BF))
            live = (rank == (q_index & 3).astype(F32)) & (((q_index >> 3) & 1) == d % 2)
            rows = slice(128 * (d % 2), 128 * (d % 2) + 128)
            cw_s[2 * a + d // 2, rows, :] = jnp.where(live, weight, 0.0).astype(BF)

    l_wg.wait()
    l_wu.wait()
    l_wd.wait()
    for n in (0, 1):
        picked = []
        for a in AXES:
            for half in (0, 1):
                plane_wait(a, half, n, send, recv, ds, dr).wait_recv()
            picked.append(dot(pick_s[a], recv[a][n].reshape(512, WIDTHS[a])).astype(BF))
        acts = []
        for j in (0, 1):
            rows = jnp.concatenate([p[256 * j : 256 * j + 256] for p in picked], axis=1)
            acts.append((silu(dot(rows, wg_s[j])) * dot(rows, wu_s[j])).astype(BF))
        for half in (1, 0):
            for a in AXES:
                rows = slice(256 * half, 256 * half + 256)
                both = jnp.concatenate(
                    [dot(place_s[a, rows, 256 * j : 256 * j + 256], acts[j]).astype(BF) for j in (0, 1)],
                    axis=1,
                )
                cols = slice(STARTS[a], STARTS[a] + WIDTHS[a])
                done = jnp.concatenate([wd_s[0, :, cols], wd_s[1, :, cols]], axis=0)
                done = dot(both, done).astype(BF).reshape(16, 16, WIDTHS[a])
                ret[a][n, half] = done
                if n == 0:
                    back[a][0, half, 0] = done[0]
            plane_copies(half, n, ret, back, es, er, -1)

    for one in b_copies.values():
        one.wait_send()
    p_copies = []
    for half in (1, 0):
        for a in AXES:
            total_a = jnp.zeros((256, WIDTHS[a]), F32)
            for n in (0, 1):
                plane_wait(a, half, n, ret, back, es, er).wait_recv()
                total_a = total_a + dot(
                    cw_s[2 * a + half, :, 256 * n : 256 * n + 256],
                    back[a][n, half].reshape(256, WIDTHS[a]),
                )
            for d in (2 * half, 2 * half + 1):
                mine = total_a[128 * (d % 2) : 128 * (d % 2) + 128]
                if d == 0:
                    cols = slice(STARTS[a], STARTS[a] + WIDTHS[a])
                    shared_s[:, cols] += mine
                else:
                    lines[a][d] = mine.astype(BF)
                    one = line_copy(a, d, lines[a].at[d], sums[a].at[d - 1], ps, pr, -1)
                    one.start()
                    p_copies.append(one)
    for one in p_copies:
        one.wait()
    for a in AXES:
        cols = slice(STARTS[a], STARTS[a] + WIDTHS[a])
        value = mid_s[:, cols].astype(F32) + shared_s[:, cols]
        for d in range(3):
            value = value + sums[a][d].astype(F32)
        out_ref[:, cols] = value.astype(BF)
    for n in (0, 1):
        for half in (0, 1):
            for a in AXES:
                plane_wait(a, half, n, send, recv, ds, dr).wait_send()
                plane_wait(a, half, n, ret, back, es, er).wait_send()


def on_device(
    queries, key_matrix, value_matrix, channel_decay_input, head_decay_offset, output_gate_input,
    head_norm_gain, residual, mixer_output_weight, expert_norm_gain, routes, chosen_router_scores,
    routed_gate_weight, routed_up_weight, routed_down_weight, common_gate_weight,
    common_up_weight, common_down_weight,
):
    any_ = pl.BlockSpec(memory_space=pl.ANY)
    vm = pl.BlockSpec(memory_space=pltpu.VMEM)
    dma = pltpu.SemaphoreType.DMA
    V = pltpu.VMEM
    return pl.pallas_call(
        kernel,
        out_shape=jax.ShapeDtypeStruct((128, 2048), BF),
        in_specs=[
            any_, any_, any_, any_, vm, any_, vm, any_, any_, vm,
            vm, vm, any_, any_, any_, any_, any_, any_,
        ],
        out_specs=vm,
        scratch_shapes=[
            V((512, 128), BF), V((512, 128), BF), V((512, 256), BF), V((512, 128), BF),
            V((512, 256), BF), V((128, 2048), BF), V((1024, 2048), BF),
            V((2, 2048, 512), BF), V((2, 2048, 512), BF), V((2, 512, 2048), BF),
            V((2048, 512), BF), V((2048, 512), BF), V((512, 2048), BF),
            V((144, 128), BF), V((144, 128), BF), V((NY, 144, 128), BF), V((NZ, 144, 128), BF),
            V((2, 512, 128), F32), V((512, 128), BF), V((4, 128, 256), BF), V((4, 128, 256), BF),
            V((128, 2048), BF), V((128, 2048), F32),
            V((12, 8, 128), F32), V((6, 512, 256), BF), V((6, 256, 512), BF),
            V((3, 512, 512), BF), V((3, 512, 512), BF),
            *[V((4, 128, w), BF) for w in WIDTHS], *[V((3, 128, w), BF) for w in WIDTHS],
            *[V((2, 2, 16, 16, w), BF) for _ in range(4) for w in WIDTHS],
            dma((13,)), dma, dma, dma((4,)), dma((4,)), dma((4,)), dma((4,)), dma((4,)), dma((4,)),
            *[dma((12,)) for _ in range(10)],
        ],
        compiler_params=pltpu.CompilerParams(
            collective_id=0, has_side_effects=True, vmem_limit_bytes=62 * 1024 * 1024
        ),
        name="layer",
    )(
        queries, key_matrix, value_matrix, channel_decay_input, head_decay_offset.T,
        output_gate_input, head_norm_gain.reshape(1, 128), residual, mixer_output_weight,
        expert_norm_gain.reshape(1, 2048), routes.T, chosen_router_scores.T, routed_gate_weight,
        routed_up_weight, routed_down_weight, common_gate_weight, common_up_weight,
        common_down_weight,
    )


def solution(mesh):
    both = ("sp", "tp")
    split, rows, rep = P("sp", "tp"), P(both, None), P()
    return jax.shard_map(
        on_device,
        mesh=mesh,
        in_specs=(
            split, split, split, split, split, split, rep, rows, rep, rep, rows, rows,
            P(both, None, None), P(both, None, None), P(both, None, None), rep, rep, rep,
        ),
        out_specs=rows,
        check_vma=False,
    )
```

```python
import jax
import jax.numpy as jnp
from jax import lax
from jax.experimental import pallas as pl
from jax.experimental.pallas import tpu as pltpu
from jax.sharding import PartitionSpec as P

MESH = pl.DeviceIdType.MESH
BF = jnp.bfloat16
F32 = jnp.float32
I32 = jnp.int32

BLOCK = 64
NZ, NY, NC, NX = 4, 4, 2, 4
DEVS = NZ * NY * NC * NX
STEP = 5
WIDTHS = (640, 640, 768)
STARTS = (0, 640, 1280)
FIRST = (384, 384, 384)
AXES = (0, 1, 2)

EPS = 1e-6
RUNNING = 16.0
SCALE = 2.5


def dot(a, b):
    return jnp.dot(a, b, preferred_element_type=F32)


def dot_nt(a, b):
    return lax.dot_general(a, b, (((1,), (1,)), ((), ())), preferred_element_type=F32)


def dot_tn(a, b):
    return lax.dot_general(a, b, (((0,), (0,)), ((), ())), preferred_element_type=F32)


def silu(v):
    return v / (1.0 + jnp.exp(-v))


def three(v):
    hi = v.astype(BF)
    rest = v - hi.astype(F32)
    mid = rest.astype(BF)
    low = (rest - mid.astype(F32)).astype(BF)
    return hi, mid, low


def kernel(
    q_hbm, k_hbm, v_hbm, cd_hbm, hd_ref, og_hbm, hgain_ref, res_hbm, wo_hbm, egain_ref,
    routes_ref, scores_ref, wg_hbm, wu_hbm, wd_hbm, cg_hbm, cu_hbm, cdn_hbm,
    out_ref,
    q_s, k_s, v_s, cd_s, og_s, res_s, wo_s, wg_s, wu_s, wd_s, cg_s, cu_s, cdn_s,
    st1, st1r, st2, st3, outacc, qx_s, gsend, grecv, mid_s, shared_s, third_s,
    rt_s, lhs_s, cw_s, pick_s, place_s,
    bx, by, bz, px, py, pz, sx, sy, sz, rx, ry, rz, tx, ty, tz, kx, ky, kz,
    load_sem, s1, r1, s2, r2, s3, r3, gs, gr,
    ts, tr, bs, br, ds, dr, es, er, ps, pr,
):
    sp = lax.axis_index("sp")
    x = lax.axis_index("tp")
    z = sp // (NY * NC)
    y = (sp // NC) % NY
    c = sp % NC

    def place(zz, yy, cc, xx):
        return ((zz % NZ) * (NY * NC) + (yy % NY) * NC + cc % NC, xx % NX)

    lines, sums = (bx, by, bz), (px, py, pz)
    send, recv, ret, back = (sx, sy, sz), (rx, ry, rz), (tx, ty, tz), (kx, ky, kz)

    def along(a, d):
        return place(z + (d if a == 2 else 0), y + (d if a == 1 else 0), c, x + (d if a == 0 else 0))

    def across(a, n, i, sign):
        k = (i * STEP) % 16
        d1, d2, dc = sign * (k // 4), sign * (k % 4), sign * n
        if a == 0:
            return place(z + NZ + d1, y + NY + d2, c + NC + dc, x)
        if a == 1:
            return place(z + NZ + d1, y, c + NC + dc, x + NX + d2)
        return place(z, y + NY + d1, c + NC + dc, x + NX + d2)

    def plane_split(i):
        k = (i * STEP) & 15
        return k >> 2, k & 3

    def expert_of(a, n, i, j):
        d1, d2 = plane_split(i)
        zz = (z + (0 if a == 2 else d1)) & 3
        yy = (y + (0 if a == 1 else (d2 if a == 0 else d1))) & 3
        xx = (x + (0 if a == 0 else d2)) & 3
        return ((zz * 8 + yy * 2 + ((c + n) & 1)) * 4 + xx) * 2 + j

    def line_copy(a, d, src, dst, ssem, rsem, sign):
        return pltpu.make_async_remote_copy(
            src_ref=src, dst_ref=dst, send_sem=ssem.at[4 * a + d], recv_sem=rsem.at[4 * a + d],
            device_id=along(a, d if sign > 0 else 4 - d), device_id_type=MESH,
        )

    loads = [
        pltpu.make_async_copy(a, b, load_sem.at[n])
        for n, (a, b) in enumerate(
            (
                (cd_hbm, cd_s), (k_hbm, k_s), (v_hbm, v_s), (q_hbm, q_s), (og_hbm, og_s),
                (wo_hbm, wo_s), (res_hbm, res_s), (cg_hbm, cg_s), (cu_hbm, cu_s),
                (cdn_hbm, cdn_s), (wg_hbm, wg_s), (wu_hbm, wu_s), (wd_hbm, wd_s),
            )
        )
    ]
    for one in loads[:5]:
        one.start()
    (l_cd, l_k, l_v, l_q, l_og, l_wo, l_res, l_cg, l_cu, l_cdn, l_wg, l_wu, l_wd) = loads

    bar = pltpu.get_barrier_semaphore()
    neighbours = [place(z, y, c + 1, x)]
    neighbours += [place(z, y + d, c, x) for d in (1, 2, 3)]
    neighbours += [place(z + d, y, c, x) for d in (1, 2, 3)]
    neighbours += [place(z, y, c, x + d) for d in (1, 2, 3)]
    for one in neighbours:
        pl.semaphore_signal(bar, inc=1, device_id=one, device_id_type=MESH)

    lane = lax.broadcasted_iota(I32, (1, 128), 1)
    first = lane < 64
    rows_i = lax.broadcasted_iota(I32, (256, 256), 0)
    cols_i = lax.broadcasted_iota(I32, (256, 256), 1)
    causal = (rows_i >= cols_i) & ((rows_i >> 6) == (cols_i >> 6))
    tri = causal.astype(F32).astype(BF)
    hd_t = jnp.concatenate([hd_ref[...], jnp.zeros((6, 512), F32)], axis=0).T
    hd = jnp.where(first, hd_t[:, 0:1], hd_t[:, 1:2])
    l_cd.wait()
    cd = cd_s[...].astype(F32)
    dl = (jnp.minimum(cd, 0.0) - jnp.log1p(jnp.exp(-jnp.abs(cd)))) / RUNNING + hd
    parts = three(dl)
    within = jnp.concatenate(
        [sum(dot(tri, p[256 * n : 256 * n + 256]) for p in parts) for n in (0, 1)], axis=0
    )
    w3 = within.reshape(8, BLOCK, 128)
    ends = [w3[n, BLOCK - 1 : BLOCK, :] for n in range(8)]
    incl = []
    running = jnp.zeros((1, 128), F32)
    for n in range(8):
        running = running + ends[n]
        incl.append(running)
    total = incl[7]
    excl3 = jnp.stack([incl[n] - ends[n] for n in range(8)], axis=0)
    ends3 = jnp.stack(ends, axis=0)

    l_k.wait()
    l_v.wait()
    k = k_s[...].astype(F32)
    k3 = k.reshape(8, BLOCK, 128)
    k_tt = (k3 * jnp.exp(total[None] - excl3 - w3)).reshape(512, 128).astype(BF)
    v0, v1 = v_s[:, 0:128], v_s[:, 128:256]
    own_state = jnp.where(first, dot_tn(v0, k_tt), dot_tn(v1, k_tt))

    row16 = lax.broadcasted_iota(I32, (16, 128), 0)

    def put_state(ref, log, state):
        ref[0:128, :] = state.astype(BF)
        hi, mid, low = (p.astype(F32) for p in three(log))
        tail = jnp.where(row16 == 0, hi, jnp.where(row16 == 1, mid, jnp.where(row16 == 2, low, 0.0)))
        ref[128:144, :] = tail.astype(BF)

    def get_state(ref):
        log = jnp.sum(ref[128:144, :].astype(F32), axis=0, keepdims=True)
        return log, ref[0:128, :].astype(F32)

    put_state(st1, total, own_state)
    scores = scores_ref[...]
    weights = SCALE * scores / jnp.sum(scores, axis=0, keepdims=True)
    rt_s[0] = jnp.concatenate([routes_ref[...].astype(F32), weights], axis=0)
    pl.semaphore_wait(bar, 10)
    core_copy = pltpu.make_async_remote_copy(
        src_ref=st1, dst_ref=st1r, send_sem=s1, recv_sem=r1,
        device_id=place(z, y, c + 1, x), device_id_type=MESH,
    )
    core_copy.start()
    rt_copies = [
        line_copy(a, d, rt_s.at[0], rt_s.at[4 * a + d], ts, tr, 1) for a in AXES for d in (1, 2, 3)
    ]
    for one in rt_copies:
        one.start()
    for one in loads[5:]:
        one.start()

    l_q.wait()
    ew = jnp.exp(within)
    qd = q_s[...].astype(F32) * 0.125 * ew
    qx_s[...] = (qd.reshape(8, BLOCK, 128) * jnp.exp(excl3)).reshape(512, 128).astype(BF)
    kg = (k * jnp.exp(-within)).astype(BF)
    for h in (0, 1):
        q_h = jnp.where(first if h == 0 else ~first, qd, 0.0).astype(BF)
        v_h = v0 if h == 0 else v1
        for n in (0, 1):
            sl = slice(256 * n, 256 * n + 256)
            scores = jnp.where(causal, dot_nt(q_h[sl], kg[sl]), 0.0).astype(BF)
            outacc[h, sl, :] = dot(scores, v_h[sl])

    core_copy.wait()
    core1 = c == 1
    log_p, state_p = get_state(st1r)
    pair_log = total + log_p
    pair_state = jnp.where(
        core1,
        jnp.exp(total) * state_p + own_state,
        jnp.exp(log_p) * own_state + state_p,
    )
    carry_log = jnp.where(core1, log_p, 0.0)
    carry_state = jnp.where(core1, state_p, 0.0)

    def exchange(slots, mine, log, state, ssem, rsem, target):
        put_state(slots.at[mine], log, state)
        copies = []
        for d in (1, 2, 3):
            one = pltpu.make_async_remote_copy(
                src_ref=slots.at[mine], dst_ref=slots.at[mine],
                send_sem=ssem.at[d], recv_sem=rsem.at[d],
                device_id=target(d), device_id_type=MESH,
            )
            one.start()
            copies.append(one)
        return copies

    def prefix(slots, mine, count, carry_log, carry_state):
        run_log = jnp.zeros((1, 128), F32)
        run_state = jnp.zeros((128, 128), F32)
        pre_log, pre_state = run_log, run_state
        for n in range(count):
            pre_log = jnp.where(mine == n, run_log, pre_log)
            pre_state = jnp.where(mine == n, run_state, pre_state)
            log, state = get_state(slots.at[n])
            run_state = jnp.exp(log) * run_state + state
            run_log = run_log + log
        carry_state = jnp.exp(carry_log) * pre_state + carry_state
        carry_log = carry_log + pre_log
        return run_log, run_state, carry_log, carry_state

    y_copies = exchange(st2, y, pair_log, pair_state, s2, r2, lambda d: place(z, y + d, c, x))

    k_tail = (k3 * jnp.exp(ends3 - w3)).reshape(512, 128).astype(BF)
    state = jnp.zeros((128, 128), F32)
    for n in range(8):
        sl = slice(BLOCK * n, BLOCK * n + BLOCK)
        if n > 0:
            state_b = state.astype(BF)
            for h in (0, 1):
                q_h = jnp.where(first if h == 0 else ~first, qd[sl], 0.0).astype(BF)
                outacc[h, sl, :] += dot_nt(q_h, state_b)
        if n < 7:
            added = jnp.where(first, dot_tn(v0[sl], k_tail[sl]), dot_tn(v1[sl], k_tail[sl]))
            state = jnp.exp(ends[n]) * state + added

    for one in y_copies:
        one.wait()
    plane_log, plane_state, carry_log, carry_state = prefix(st2, y, NY, carry_log, carry_state)
    z_copies = exchange(st3, z, plane_log, plane_state, s3, r3, lambda d: place(z + d, y, c, x))

    for one in rt_copies:
        one.wait()
    sub128 = lax.broadcasted_iota(I32, (128, 128), 0)
    lan128 = lax.broadcasted_iota(I32, (128, 128), 1)
    upper = (sub128 < lan128).astype(F32).astype(BF)
    lower = (sub128 > lan128).astype(F32).astype(BF)
    nothing = jnp.zeros((32, 8, 128), F32)
    q_index = lax.broadcasted_iota(I32, (256, 128), 0)
    for a in AXES:
        expert = expert_of(a, q_index >> 7, (q_index >> 3) & 15, (q_index >> 2) & 1).astype(F32)
        for d in range(4):
            info = rt_s[4 * a + d if d else 0]
            match = jnp.zeros((256, 128), F32)
            for j in range(4):
                match = jnp.where(expert == info[j : j + 1, :], 1.0, match)
            rank = dot(match.astype(BF), upper)
            live = jnp.where(rank == (q_index & 3).astype(F32), match, 0.0).reshape(32, 8, 128)
            pair = [live, nothing] if d % 2 == 0 else [nothing, live]
            cols = slice(128 * (d % 2), 128 * (d % 2) + 128)
            lhs_s[2 * a + d // 2, :, cols] = (
                jnp.concatenate(pair, axis=1).reshape(512, 128).astype(BF)
            )

    for one in z_copies:
        one.wait()
    _, _, _, carried = prefix(st3, z, NZ, carry_log, carry_state)
    carried_b = carried.astype(BF)

    l_og.wait()
    g_copies = []
    for d in (1, 2, 3, 0):
        xx = (x + d) % NX
        rows = pl.ds(pl.multiple_of(xx * 128, 128), 128)
        qx = qx_s[rows, :]
        for h in (0, 1):
            q_h = jnp.where(first if h == 0 else ~first, qx.astype(F32), 0.0).astype(BF)
            attn = outacc[h, rows, :] + dot_nt(q_h, carried_b)
            inv = lax.rsqrt(jnp.mean(attn * attn, axis=-1, keepdims=True) + EPS)
            gate = og_s[rows, 128 * h : 128 * h + 128].astype(F32)
            value = attn * inv * hgain_ref[...] * silu(gate)
            gsend[d, :, 128 * h : 128 * h + 128] = value.astype(BF)
        if d > 0:
            one = pltpu.make_async_remote_copy(
                src_ref=gsend.at[d], dst_ref=grecv.at[d], send_sem=gs.at[d], recv_sem=gr.at[d],
                device_id=place(z, y, c, x + d), device_id_type=MESH,
            )
            one.start()
            g_copies.append(one)

    l_wo.wait()
    l_res.wait()
    w_rows = pl.ds(pl.multiple_of(x * 256, 256), 256)
    proj = dot(gsend[0], wo_s[w_rows, :])
    for d in (1, 2, 3):
        g_copies[d - 1].wait()
        w_rows = pl.ds(pl.multiple_of(((x + NX - d) % NX) * 256, 256), 256)
        proj = proj + dot(grecv[d], wo_s[w_rows, :])
    middle = (res_s[...].astype(F32) + proj).astype(BF)
    mid_s[...] = middle
    mid_w = middle.astype(F32)
    scale = lax.rsqrt(jnp.mean(mid_w * mid_w, axis=-1, keepdims=True) + EPS)
    normed = (mid_w * scale * egain_ref[...]).astype(BF)
    def columns(a, part):
        return slice(0, FIRST[a]) if part == 0 else slice(FIRST[a], WIDTHS[a])

    def relay(a, part, source, dest, ssem, rsem, toward):
        cols = columns(a, part)
        return pltpu.make_async_remote_copy(
            src_ref=source.at[:, cols], dst_ref=dest.at[:, cols],
            send_sem=ssem, recv_sem=rsem,
            device_id=along(a, toward), device_id_type=MESH,
        )

    b_copies = {}
    for a in AXES:
        lines[a][0] = normed[:, STARTS[a] : STARTS[a] + WIDTHS[a]]
        for part in (0, 1):
            for d in (1, 3):
                n = 8 * a + 2 * part + d // 2
                b_copies[a, d, part] = relay(
                    a, part, lines[a].at[0], lines[a].at[d], bs.at[n], br.at[n], d
                )
            n, d = 8 * a + 4 + part, 1 + 2 * part
            b_copies[a, 2, part] = relay(
                a, part, lines[a].at[d], lines[a].at[2], bs.at[n], br.at[n], d
            )
    for part in (0, 1):
        for d in (1, 3):
            for a in AXES:
                b_copies[a, d, part].start()

    def sem(a, half, n):
        return 4 * a + 2 * half + n

    def plane_copies(half, n, source, dest, ssem, rsem, sign):
        def body(i, carry):
            for a in AXES:
                pltpu.make_async_remote_copy(
                    src_ref=source[a].at[n, half, i], dst_ref=dest[a].at[n, half, i],
                    send_sem=ssem.at[sem(a, half, n)], recv_sem=rsem.at[sem(a, half, n)],
                    device_id=across(a, n, i, sign), device_id_type=MESH,
                ).start()
            return carry

        lax.fori_loop(1 if n == 0 else 0, 16, body, 0)

    def split_copy(n, a, part, i, source, dest, ssem, rsem, sign):
        at = sem(a, 0, n) if part == 0 else 12 + a
        cols = columns(a, part)
        return pltpu.make_async_remote_copy(
            src_ref=source[a].at[n, 0, i, :, cols], dst_ref=dest[a].at[n, 0, i, :, cols],
            send_sem=ssem.at[at], recv_sem=rsem.at[at],
            device_id=across(a, 1, 1, sign) if isinstance(i, slice) else across(a, n, i, sign),
            device_id_type=MESH,
        )

    def split_copies(n, part, source, dest, ssem, rsem, sign):
        def body(i, carry):
            for a in AXES:
                split_copy(n, a, part, i, source, dest, ssem, rsem, sign).start()
            return carry

        lax.fori_loop(1 if n == 0 else 0, 16, body, 0)

    def out_wait(a, part):
        return split_copy(0, a, part, slice(1, 16), send, recv, ds, dr, 1)

    def last_wait(a, part):
        return split_copy(1, a, part, slice(0, 16), ret, back, es, er, -1)

    def plane_wait(a, half, n, source, dest, ssem, rsem):
        part = pl.ds(1, 15) if n == 0 else pl.ds(0, 16)
        return pltpu.make_async_remote_copy(
            src_ref=source[a].at[n, half, part], dst_ref=dest[a].at[n, half, part],
            send_sem=ssem.at[sem(a, half, n)], recv_sem=rsem.at[sem(a, half, n)],
            device_id=across(a, 1, 1, 1), device_id_type=MESH,
        )

    for part in (0, 1):
        for a in AXES:
            b_copies[a, 1, part].wait_recv()
            if part == 1:
                b_copies[a, 3, 1].wait_recv()
            b_copies[a, 2, part].start()
        for a in AXES:
            cols = columns(a, part)
            wide = cols.stop - cols.start
            rows = dot(lhs_s[2 * a, 0:256, :], lines[a][0:2, :, cols].reshape(256, wide))
            rows = rows.astype(BF).reshape(16, 16, wide)
            send[a][0, 0, :, :, cols] = rows
            recv[a][0, 0, 0, :, cols] = rows[0]
        split_copies(0, part, send, recv, ds, dr, 1)
    for n, half in ((0, 1), (1, 0), (1, 1)):
        for a in AXES:
            if n == 0:
                b_copies[a, 3, 0].wait_recv()
                b_copies[a, 2, 0].wait_recv()
                b_copies[a, 2, 1].wait_recv()
            rows = dot(
                lhs_s[2 * a + half, 256 * n : 256 * n + 256, :],
                lines[a][2 * half : 2 * half + 2].reshape(256, WIDTHS[a]),
            ).astype(BF).reshape(16, 16, WIDTHS[a])
            send[a][n, half] = rows
            if n == 0:
                recv[a][0, half, 0] = rows[0]
        plane_copies(half, n, send, recv, ds, dr, 1)

    l_cg.wait()
    l_cu.wait()
    l_cdn.wait()
    nrm = jnp.concatenate([lines[a][0] for a in AXES], axis=1)
    hidden = (silu(dot(nrm, cg_s[...])) * dot(nrm, cu_s[...])).astype(BF)
    shared_s[...] = dot(hidden, cdn_s[...])

    def row_of(a, q):
        d1, d2 = plane_split((q >> 4) & 15)
        d = ((q >> 8) & 1) * 2 + ((q >> 3) & 1)
        dz, dy, dx = ((d1, d2, d), (d1, d, d2), (d, d1, d2))[a]
        return ((q >> 2) & 1) * 256 + (dz * 16 + dy * 4 + dx) * 4 + (q & 3)

    down = lax.broadcasted_iota(I32, (512, 512), 0)
    over = lax.broadcasted_iota(I32, (512, 512), 1)
    for a in AXES:
        pick_s[a] = (down == row_of(a, over)).astype(F32).astype(BF)
        place_s[a] = (over == row_of(a, down)).astype(F32).astype(BF)
    q_index = lax.broadcasted_iota(I32, (128, 512), 1)
    blank = jnp.zeros((120, 128), F32)
    for a in AXES:
        expert = expert_of(a, q_index >> 8, (q_index >> 4) & 15, (q_index >> 2) & 1).astype(F32)
        for d in range(4):
            info = jnp.concatenate([rt_s[4 * a + d if d else 0], blank], axis=0).T
            weight = jnp.zeros((128, 512), F32)
            match = jnp.zeros((128, 512), F32)
            for j in range(4):
                hit = expert == info[:, j : j + 1]
                match = jnp.where(hit, 1.0, match)
                weight = jnp.where(hit, info[:, 4 + j : 5 + j], weight)
            rank = dot(lower, match.astype(BF))
            live = (rank == (q_index & 3).astype(F32)) & (((q_index >> 3) & 1) == d % 2)
            rows = slice(128 * (d % 2), 128 * (d % 2) + 128)
            cw_s[2 * a + d // 2, rows, :] = jnp.where(live, weight, 0.0).astype(BF)

    l_wg.wait()
    l_wu.wait()
    l_wd.wait()
    for n in (0, 1):
        picked = []
        for a in AXES:
            for half in (0, 1):
                if (n, half) == (0, 0):
                    out_wait(a, 0).wait_recv()
                    out_wait(a, 1).wait_recv()
                else:
                    plane_wait(a, half, n, send, recv, ds, dr).wait_recv()
            picked.append(dot(pick_s[a], recv[a][n].reshape(512, WIDTHS[a])).astype(BF))
        acts = []
        for j in (0, 1):
            rows = jnp.concatenate([p[256 * j : 256 * j + 256] for p in picked], axis=1)
            acts.append((silu(dot(rows, wg_s[j])) * dot(rows, wu_s[j])).astype(BF))
        for half in (1, 0):
            for a in AXES:
                rows = slice(256 * half, 256 * half + 256)
                both = jnp.concatenate(
                    [dot(place_s[a, rows, 256 * j : 256 * j + 256], acts[j]).astype(BF) for j in (0, 1)],
                    axis=1,
                )
                cols = slice(STARTS[a], STARTS[a] + WIDTHS[a])
                done = jnp.concatenate([wd_s[0, :, cols], wd_s[1, :, cols]], axis=0)
                done = dot(both, done).astype(BF).reshape(16, 16, WIDTHS[a])
                ret[a][n, half] = done
                if n == 0:
                    back[a][0, half, 0] = done[0]
            if (n, half) == (1, 0):
                split_copies(1, 0, ret, back, es, er, -1)
            else:
                plane_copies(half, n, ret, back, es, er, -1)

    for one in b_copies.values():
        one.wait_send()
    p_copies = []

    def plane_sum(a, half, cols):
        return sum(
            dot(
                cw_s[2 * a + half, :, 256 * n : 256 * n + 256],
                back[a][n, half, :, :, cols].reshape(256, cols.stop - cols.start),
            )
            for n in (0, 1)
        )

    for a in AXES:
        for n in (0, 1):
            plane_wait(a, 1, n, ret, back, es, er).wait_recv()
        sum_a = plane_sum(a, 1, slice(0, WIDTHS[a]))
        lines[a][2] = sum_a[0:128].astype(BF)
        third_s[:, STARTS[a] : STARTS[a] + WIDTHS[a]] = sum_a[128:256]
        for part, toward in ((0, 3), (1, 1)):
            one = relay(
                a, part, lines[a].at[2], sums[a].at[1], ps.at[8 * a + part], pr.at[8 * a + part],
                toward,
            )
            one.start()
            p_copies.append(one)
    relayed = list(p_copies)
    split_copies(1, 1, ret, back, es, er, -1)
    for part in (0, 1):
        for a in AXES:
            cols = columns(a, part)
            whole = slice(STARTS[a] + cols.start, STARTS[a] + cols.stop)
            if part == 0:
                plane_wait(a, 0, 0, ret, back, es, er).wait_recv()
            last_wait(a, part).wait_recv()
            sum_a = plane_sum(a, 0, cols)
            shared_s[:, whole] += sum_a[0:128]
            value = sum_a[128:256]
            if part == 0:
                relayed[2 * a].wait_recv()
                value = value + sums[a][1, :, cols].astype(F32)
            lines[a][1, :, cols] = value.astype(BF)
            one = relay(
                a, part, lines[a].at[1], sums[a].at[0], ps.at[8 * a + 2 + part],
                pr.at[8 * a + 2 + part], 3,
            )
            one.start()
            p_copies.append(one)
        if part == 0:
            for a in AXES:
                cols = slice(FIRST[a], WIDTHS[a])
                relayed[2 * a + 1].wait_recv()
                value = third_s[:, STARTS[a] : STARTS[a] + WIDTHS[a]]
                lines[a][3, :, 0 : FIRST[a]] = value[:, 0 : FIRST[a]].astype(BF)
                lines[a][3, :, cols] = (value[:, cols] + sums[a][1, :, cols].astype(F32)).astype(BF)
                one = pltpu.make_async_remote_copy(
                    src_ref=lines[a].at[3], dst_ref=sums[a].at[2],
                    send_sem=ps.at[8 * a + 4], recv_sem=pr.at[8 * a + 4],
                    device_id=along(a, 1), device_id_type=MESH,
                )
                one.start()
                p_copies.append(one)
    for one in p_copies:
        if not any(one is r for r in relayed):
            one.wait_recv()
    for a in AXES:
        cols = slice(STARTS[a], STARTS[a] + WIDTHS[a])
        value = mid_s[:, cols].astype(F32) + shared_s[:, cols]
        value = value + sums[a][0].astype(F32) + sums[a][2].astype(F32)
        out_ref[:, cols] = value.astype(BF)
    for one in p_copies:
        one.wait_send()
    for n in (0, 1):
        for half in (0, 1):
            for a in AXES:
                if (n, half) == (0, 0):
                    out_wait(a, 0).wait_send()
                    out_wait(a, 1).wait_send()
                else:
                    plane_wait(a, half, n, send, recv, ds, dr).wait_send()
                if (n, half) == (1, 0):
                    last_wait(a, 0).wait_send()
                    last_wait(a, 1).wait_send()
                else:
                    plane_wait(a, half, n, ret, back, es, er).wait_send()


def on_device(
    queries, key_matrix, value_matrix, channel_decay_input, head_decay_offset, output_gate_input,
    head_norm_gain, residual, mixer_output_weight, expert_norm_gain, routes, chosen_router_scores,
    routed_gate_weight, routed_up_weight, routed_down_weight, common_gate_weight,
    common_up_weight, common_down_weight,
):
    any_ = pl.BlockSpec(memory_space=pl.ANY)
    vm = pl.BlockSpec(memory_space=pltpu.VMEM)
    dma = pltpu.SemaphoreType.DMA
    V = pltpu.VMEM
    return pl.pallas_call(
        kernel,
        out_shape=jax.ShapeDtypeStruct((128, 2048), BF),
        in_specs=[
            any_, any_, any_, any_, vm, any_, vm, any_, any_, vm,
            vm, vm, any_, any_, any_, any_, any_, any_,
        ],
        out_specs=vm,
        scratch_shapes=[
            V((512, 128), BF), V((512, 128), BF), V((512, 256), BF), V((512, 128), BF),
            V((512, 256), BF), V((128, 2048), BF), V((1024, 2048), BF),
            V((2, 2048, 512), BF), V((2, 2048, 512), BF), V((2, 512, 2048), BF),
            V((2048, 512), BF), V((2048, 512), BF), V((512, 2048), BF),
            V((144, 128), BF), V((144, 128), BF), V((NY, 144, 128), BF), V((NZ, 144, 128), BF),
            V((2, 512, 128), F32), V((512, 128), BF), V((4, 128, 256), BF), V((4, 128, 256), BF),
            V((128, 2048), BF), V((128, 2048), F32), V((128, 2048), F32),
            V((12, 8, 128), F32), V((6, 512, 256), BF), V((6, 256, 512), BF),
            V((3, 512, 512), BF), V((3, 512, 512), BF),
            *[V((4, 128, w), BF) for w in WIDTHS], *[V((3, 128, w), BF) for w in WIDTHS],
            *[V((2, 2, 16, 16, w), BF) for _ in range(4) for w in WIDTHS],
            dma((13,)), dma, dma, dma((4,)), dma((4,)), dma((4,)), dma((4,)), dma((4,)), dma((4,)),
            dma((12,)), dma((12,)), dma((24,)), dma((24,)), *[dma((15,)) for _ in range(4)],
            dma((24,)), dma((24,)),
        ],
        compiler_params=pltpu.CompilerParams(
            collective_id=0, has_side_effects=True, vmem_limit_bytes=62 * 1024 * 1024
        ),
        name="layer",
    )(
        queries, key_matrix, value_matrix, channel_decay_input, head_decay_offset.T,
        output_gate_input, head_norm_gain.reshape(1, 128), residual, mixer_output_weight,
        expert_norm_gain.reshape(1, 2048), routes.T, chosen_router_scores.T, routed_gate_weight,
        routed_up_weight, routed_down_weight, common_gate_weight, common_up_weight,
        common_down_weight,
    )


def solution(mesh):
    both = ("sp", "tp")
    split, rows, rep = P("sp", "tp"), P(both, None), P()
    return jax.shard_map(
        on_device,
        mesh=mesh,
        in_specs=(
            split, split, split, split, split, split, rep, rows, rep, rep, rows, rows,
            P(both, None, None), P(both, None, None), P(both, None, None), rep, rep, rep,
        ),
        out_specs=rows,
        check_vma=False,
    )
```

```python
import jax
import jax.numpy as jnp
from jax import lax
from jax.experimental import pallas as pl
from jax.experimental.pallas import tpu as pltpu
from jax.sharding import PartitionSpec as P

MESH = pl.DeviceIdType.MESH
BF = jnp.bfloat16
F32 = jnp.float32
I32 = jnp.int32

BLOCK = 64
NZ, NY, NC, NX = 4, 4, 2, 4
DEVS = NZ * NY * NC * NX
STEP = 11
WIDTHS = (640, 640, 768)
STARTS = (0, 640, 1280)
FIRST = (384, 384, 384)
AXES = (0, 1, 2)

EPS = 1e-6
RUNNING = 16.0
SCALE = 2.5


def dot(a, b):
    return jnp.dot(a, b, preferred_element_type=F32)


def dot_nt(a, b):
    return lax.dot_general(a, b, (((1,), (1,)), ((), ())), preferred_element_type=F32)


def dot_tn(a, b):
    return lax.dot_general(a, b, (((0,), (0,)), ((), ())), preferred_element_type=F32)


def silu(v):
    return v / (1.0 + jnp.exp(-v))


def three(v):
    hi = v.astype(BF)
    rest = v - hi.astype(F32)
    mid = rest.astype(BF)
    low = (rest - mid.astype(F32)).astype(BF)
    return hi, mid, low


def kernel(
    q_hbm, k_hbm, v_hbm, cd_hbm, hd_ref, og_hbm, hgain_ref, res_hbm, wo_hbm, egain_ref,
    routes_ref, scores_ref, wg_hbm, wu_hbm, wd_hbm, cg_hbm, cu_hbm, cdn_hbm,
    out_ref,
    q_s, k_s, v_s, cd_s, og_s, res_s, wo_s, wg_s, wu_s, wd_s, cg_s, cu_s, cdn_s,
    st1, st1r, st2, st3, outacc, qx_s, gsend, grecv, mid_s, shared_s, third_s,
    rt_s, lhs_s, cw_s, pick_s, place_s,
    bx, by, bz, px, py, pz, sx, sy, sz, rx, ry, rz, tx, ty, tz, kx, ky, kz,
    load_sem, s1, r1, s2, r2, s3, r3, gs, gr,
    ts, tr, bs, br, ds, dr, es, er, ps, pr,
):
    sp = lax.axis_index("sp")
    x = lax.axis_index("tp")
    z = sp // (NY * NC)
    y = (sp // NC) % NY
    c = sp % NC

    def place(zz, yy, cc, xx):
        return ((zz % NZ) * (NY * NC) + (yy % NY) * NC + cc % NC, xx % NX)

    lines, sums = (bx, by, bz), (px, py, pz)
    send, recv, ret, back = (sx, sy, sz), (rx, ry, rz), (tx, ty, tz), (kx, ky, kz)

    def along(a, d):
        return place(z + (d if a == 2 else 0), y + (d if a == 1 else 0), c, x + (d if a == 0 else 0))

    def across(a, n, i, sign):
        k = (i * STEP) % 16
        d1, d2, dc = sign * (k // 4), sign * (k % 4), sign * n
        if a == 0:
            return place(z + NZ + d1, y + NY + d2, c + NC + dc, x)
        if a == 1:
            return place(z + NZ + d1, y, c + NC + dc, x + NX + d2)
        return place(z, y + NY + d1, c + NC + dc, x + NX + d2)

    def plane_split(i):
        k = (i * STEP) & 15
        return k >> 2, k & 3

    def expert_of(a, n, i, j):
        d1, d2 = plane_split(i)
        zz = (z + (0 if a == 2 else d1)) & 3
        yy = (y + (0 if a == 1 else (d2 if a == 0 else d1))) & 3
        xx = (x + (0 if a == 0 else d2)) & 3
        return ((zz * 8 + yy * 2 + ((c + n) & 1)) * 4 + xx) * 2 + j

    def line_copy(a, d, src, dst, ssem, rsem, sign):
        return pltpu.make_async_remote_copy(
            src_ref=src, dst_ref=dst, send_sem=ssem.at[4 * a + d], recv_sem=rsem.at[4 * a + d],
            device_id=along(a, d if sign > 0 else 4 - d), device_id_type=MESH,
        )

    loads = [
        pltpu.make_async_copy(a, b, load_sem.at[n])
        for n, (a, b) in enumerate(
            (
                (cd_hbm, cd_s), (k_hbm, k_s), (v_hbm, v_s), (q_hbm, q_s), (og_hbm, og_s),
                (wo_hbm, wo_s), (res_hbm, res_s), (cg_hbm, cg_s), (cu_hbm, cu_s),
                (cdn_hbm, cdn_s), (wg_hbm, wg_s), (wu_hbm, wu_s), (wd_hbm, wd_s),
            )
        )
    ]
    for one in loads[:5]:
        one.start()
    (l_cd, l_k, l_v, l_q, l_og, l_wo, l_res, l_cg, l_cu, l_cdn, l_wg, l_wu, l_wd) = loads

    bar = pltpu.get_barrier_semaphore()
    neighbours = [place(z, y, c + 1, x)]
    neighbours += [place(z, y + d, c, x) for d in (1, 2, 3)]
    neighbours += [place(z + d, y, c, x) for d in (1, 2, 3)]
    neighbours += [place(z, y, c, x + d) for d in (1, 2, 3)]
    for one in neighbours:
        pl.semaphore_signal(bar, inc=1, device_id=one, device_id_type=MESH)

    lane = lax.broadcasted_iota(I32, (1, 128), 1)
    first = lane < 64
    rows_i = lax.broadcasted_iota(I32, (256, 256), 0)
    cols_i = lax.broadcasted_iota(I32, (256, 256), 1)
    causal = (rows_i >= cols_i) & ((rows_i >> 6) == (cols_i >> 6))
    tri = causal.astype(F32).astype(BF)
    hd_t = jnp.concatenate([hd_ref[...], jnp.zeros((6, 512), F32)], axis=0).T
    hd = jnp.where(first, hd_t[:, 0:1], hd_t[:, 1:2])
    l_cd.wait()
    cd = cd_s[...].astype(F32)
    dl = (jnp.minimum(cd, 0.0) - jnp.log1p(jnp.exp(-jnp.abs(cd)))) / RUNNING + hd
    parts = three(dl)
    within = jnp.concatenate(
        [sum(dot(tri, p[256 * n : 256 * n + 256]) for p in parts) for n in (0, 1)], axis=0
    )
    w3 = within.reshape(8, BLOCK, 128)
    ends = [w3[n, BLOCK - 1 : BLOCK, :] for n in range(8)]
    incl = []
    running = jnp.zeros((1, 128), F32)
    for n in range(8):
        running = running + ends[n]
        incl.append(running)
    total = incl[7]
    excl3 = jnp.stack([incl[n] - ends[n] for n in range(8)], axis=0)
    ends3 = jnp.stack(ends, axis=0)

    l_k.wait()
    l_v.wait()
    k = k_s[...].astype(F32)
    k3 = k.reshape(8, BLOCK, 128)
    k_tt = (k3 * jnp.exp(total[None] - excl3 - w3)).reshape(512, 128).astype(BF)
    v0, v1 = v_s[:, 0:128], v_s[:, 128:256]
    own_state = jnp.where(first, dot_tn(v0, k_tt), dot_tn(v1, k_tt))

    row16 = lax.broadcasted_iota(I32, (16, 128), 0)

    def put_state(ref, log, state):
        ref[0:128, :] = state.astype(BF)
        hi, mid, low = (p.astype(F32) for p in three(log))
        tail = jnp.where(row16 == 0, hi, jnp.where(row16 == 1, mid, jnp.where(row16 == 2, low, 0.0)))
        ref[128:144, :] = tail.astype(BF)

    def get_state(ref):
        log = jnp.sum(ref[128:144, :].astype(F32), axis=0, keepdims=True)
        return log, ref[0:128, :].astype(F32)

    put_state(st1, total, own_state)
    scores = scores_ref[...]
    weights = SCALE * scores / jnp.sum(scores, axis=0, keepdims=True)
    rt_s[0] = jnp.concatenate([routes_ref[...].astype(F32), weights], axis=0)
    pl.semaphore_wait(bar, 10)
    core_copy = pltpu.make_async_remote_copy(
        src_ref=st1, dst_ref=st1r, send_sem=s1, recv_sem=r1,
        device_id=place(z, y, c + 1, x), device_id_type=MESH,
    )
    core_copy.start()
    rt_copies = [
        line_copy(a, d, rt_s.at[0], rt_s.at[4 * a + d], ts, tr, 1) for a in AXES for d in (1, 2, 3)
    ]
    for one in rt_copies:
        one.start()
    for one in loads[5:]:
        one.start()

    l_q.wait()
    ew = jnp.exp(within)
    qd = q_s[...].astype(F32) * 0.125 * ew
    qx_s[...] = (qd.reshape(8, BLOCK, 128) * jnp.exp(excl3)).reshape(512, 128).astype(BF)
    kg = (k * jnp.exp(-within)).astype(BF)
    for h in (0, 1):
        q_h = jnp.where(first if h == 0 else ~first, qd, 0.0).astype(BF)
        v_h = v0 if h == 0 else v1
        for n in (0, 1):
            sl = slice(256 * n, 256 * n + 256)
            scores = jnp.where(causal, dot_nt(q_h[sl], kg[sl]), 0.0).astype(BF)
            outacc[h, sl, :] = dot(scores, v_h[sl])

    core_copy.wait()
    core1 = c == 1
    log_p, state_p = get_state(st1r)
    pair_log = total + log_p
    pair_state = jnp.where(
        core1,
        jnp.exp(total) * state_p + own_state,
        jnp.exp(log_p) * own_state + state_p,
    )
    carry_log = jnp.where(core1, log_p, 0.0)
    carry_state = jnp.where(core1, state_p, 0.0)

    def exchange(slots, mine, log, state, ssem, rsem, target):
        put_state(slots.at[mine], log, state)
        copies = []
        for d in (1, 2, 3):
            one = pltpu.make_async_remote_copy(
                src_ref=slots.at[mine], dst_ref=slots.at[mine],
                send_sem=ssem.at[d], recv_sem=rsem.at[d],
                device_id=target(d), device_id_type=MESH,
            )
            one.start()
            copies.append(one)
        return copies

    def prefix(slots, mine, count, carry_log, carry_state):
        run_log = jnp.zeros((1, 128), F32)
        run_state = jnp.zeros((128, 128), F32)
        pre_log, pre_state = run_log, run_state
        for n in range(count):
            pre_log = jnp.where(mine == n, run_log, pre_log)
            pre_state = jnp.where(mine == n, run_state, pre_state)
            log, state = get_state(slots.at[n])
            run_state = jnp.exp(log) * run_state + state
            run_log = run_log + log
        carry_state = jnp.exp(carry_log) * pre_state + carry_state
        carry_log = carry_log + pre_log
        return run_log, run_state, carry_log, carry_state

    y_copies = exchange(st2, y, pair_log, pair_state, s2, r2, lambda d: place(z, y + d, c, x))

    k_tail = (k3 * jnp.exp(ends3 - w3)).reshape(512, 128).astype(BF)
    state = jnp.zeros((128, 128), F32)
    for n in range(8):
        sl = slice(BLOCK * n, BLOCK * n + BLOCK)
        if n > 0:
            state_b = state.astype(BF)
            for h in (0, 1):
                q_h = jnp.where(first if h == 0 else ~first, qd[sl], 0.0).astype(BF)
                outacc[h, sl, :] += dot_nt(q_h, state_b)
        if n < 7:
            added = jnp.where(first, dot_tn(v0[sl], k_tail[sl]), dot_tn(v1[sl], k_tail[sl]))
            state = jnp.exp(ends[n]) * state + added

    for one in y_copies:
        one.wait()
    plane_log, plane_state, carry_log, carry_state = prefix(st2, y, NY, carry_log, carry_state)
    z_copies = exchange(st3, z, plane_log, plane_state, s3, r3, lambda d: place(z + d, y, c, x))

    for one in rt_copies:
        one.wait()
    sub128 = lax.broadcasted_iota(I32, (128, 128), 0)
    lan128 = lax.broadcasted_iota(I32, (128, 128), 1)
    upper = (sub128 < lan128).astype(F32).astype(BF)
    lower = (sub128 > lan128).astype(F32).astype(BF)
    nothing = jnp.zeros((32, 8, 128), F32)
    q_index = lax.broadcasted_iota(I32, (256, 128), 0)
    for a in AXES:
        expert = expert_of(a, q_index >> 7, (q_index >> 3) & 15, (q_index >> 2) & 1).astype(F32)
        for d in range(4):
            info = rt_s[4 * a + d if d else 0]
            match = jnp.zeros((256, 128), F32)
            for j in range(4):
                match = jnp.where(expert == info[j : j + 1, :], 1.0, match)
            rank = dot(match.astype(BF), upper)
            live = jnp.where(rank == (q_index & 3).astype(F32), match, 0.0).reshape(32, 8, 128)
            pair = [live, nothing] if d % 2 == 0 else [nothing, live]
            cols = slice(128 * (d % 2), 128 * (d % 2) + 128)
            lhs_s[2 * a + d // 2, :, cols] = (
                jnp.concatenate(pair, axis=1).reshape(512, 128).astype(BF)
            )

    for one in z_copies:
        one.wait()
    _, _, _, carried = prefix(st3, z, NZ, carry_log, carry_state)
    carried_b = carried.astype(BF)

    l_og.wait()
    g_copies = []
    for d in (1, 2, 3, 0):
        xx = (x + d) % NX
        rows = pl.ds(pl.multiple_of(xx * 128, 128), 128)
        qx = qx_s[rows, :]
        for h in (0, 1):
            q_h = jnp.where(first if h == 0 else ~first, qx.astype(F32), 0.0).astype(BF)
            attn = outacc[h, rows, :] + dot_nt(q_h, carried_b)
            inv = lax.rsqrt(jnp.mean(attn * attn, axis=-1, keepdims=True) + EPS)
            gate = og_s[rows, 128 * h : 128 * h + 128].astype(F32)
            value = attn * inv * hgain_ref[...] * silu(gate)
            gsend[d, :, 128 * h : 128 * h + 128] = value.astype(BF)
        if d > 0:
            one = pltpu.make_async_remote_copy(
                src_ref=gsend.at[d], dst_ref=grecv.at[d], send_sem=gs.at[d], recv_sem=gr.at[d],
                device_id=place(z, y, c, x + d), device_id_type=MESH,
            )
            one.start()
            g_copies.append(one)

    l_wo.wait()
    l_res.wait()
    w_rows = pl.ds(pl.multiple_of(x * 256, 256), 256)
    proj = dot(gsend[0], wo_s[w_rows, :])
    for d in (1, 2, 3):
        g_copies[d - 1].wait()
        w_rows = pl.ds(pl.multiple_of(((x + NX - d) % NX) * 256, 256), 256)
        proj = proj + dot(grecv[d], wo_s[w_rows, :])
    middle = (res_s[...].astype(F32) + proj).astype(BF)
    mid_s[...] = middle
    mid_w = middle.astype(F32)
    scale = lax.rsqrt(jnp.mean(mid_w * mid_w, axis=-1, keepdims=True) + EPS)
    normed = (mid_w * scale * egain_ref[...]).astype(BF)
    def columns(a, part):
        return slice(0, FIRST[a]) if part == 0 else slice(FIRST[a], WIDTHS[a])

    def relay(a, part, source, dest, ssem, rsem, toward):
        cols = columns(a, part)
        return pltpu.make_async_remote_copy(
            src_ref=source.at[:, cols], dst_ref=dest.at[:, cols],
            send_sem=ssem, recv_sem=rsem,
            device_id=along(a, toward), device_id_type=MESH,
        )

    b_copies = {}
    for a in AXES:
        lines[a][0] = normed[:, STARTS[a] : STARTS[a] + WIDTHS[a]]
        for part in (0, 1):
            for d in (1, 3):
                n = 8 * a + 2 * part + d // 2
                b_copies[a, d, part] = relay(
                    a, part, lines[a].at[0], lines[a].at[d], bs.at[n], br.at[n], d
                )
            n, d = 8 * a + 4 + part, 1 + 2 * part
            b_copies[a, 2, part] = relay(
                a, part, lines[a].at[d], lines[a].at[2], bs.at[n], br.at[n], d
            )
    for part in (0, 1):
        for d in (1, 3):
            for a in AXES:
                b_copies[a, d, part].start()

    def sem(a, half, n):
        return 4 * a + 2 * half + n

    def plane_copies(half, n, source, dest, ssem, rsem, sign):
        def body(i, carry):
            for a in AXES:
                pltpu.make_async_remote_copy(
                    src_ref=source[a].at[n, half, i], dst_ref=dest[a].at[n, half, i],
                    send_sem=ssem.at[sem(a, half, n)], recv_sem=rsem.at[sem(a, half, n)],
                    device_id=across(a, n, i, sign), device_id_type=MESH,
                ).start()
            return carry

        lax.fori_loop(1 if n == 0 else 0, 16, body, 0)

    def split_copy(n, a, part, i, source, dest, ssem, rsem, sign):
        at = sem(a, 0, n) if part == 0 else 12 + a
        cols = columns(a, part)
        return pltpu.make_async_remote_copy(
            src_ref=source[a].at[n, 0, i, :, cols], dst_ref=dest[a].at[n, 0, i, :, cols],
            send_sem=ssem.at[at], recv_sem=rsem.at[at],
            device_id=across(a, 1, 1, sign) if isinstance(i, slice) else across(a, n, i, sign),
            device_id_type=MESH,
        )

    def split_copies(n, part, source, dest, ssem, rsem, sign):
        def body(i, carry):
            for a in AXES:
                split_copy(n, a, part, i, source, dest, ssem, rsem, sign).start()
            return carry

        lax.fori_loop(1 if n == 0 else 0, 16, body, 0)

    def out_wait(a, part):
        return split_copy(0, a, part, slice(1, 16), send, recv, ds, dr, 1)

    def last_wait(a, part):
        return split_copy(1, a, part, slice(0, 16), ret, back, es, er, -1)

    def plane_wait(a, half, n, source, dest, ssem, rsem):
        part = pl.ds(1, 15) if n == 0 else pl.ds(0, 16)
        return pltpu.make_async_remote_copy(
            src_ref=source[a].at[n, half, part], dst_ref=dest[a].at[n, half, part],
            send_sem=ssem.at[sem(a, half, n)], recv_sem=rsem.at[sem(a, half, n)],
            device_id=across(a, 1, 1, 1), device_id_type=MESH,
        )

    for part in (0, 1):
        for a in AXES:
            b_copies[a, 1, part].wait_recv()
            if part == 1:
                b_copies[a, 3, 1].wait_recv()
            b_copies[a, 2, part].start()
        for a in AXES:
            cols = columns(a, part)
            wide = cols.stop - cols.start
            rows = dot(lhs_s[2 * a, 0:256, :], lines[a][0:2, :, cols].reshape(256, wide))
            rows = rows.astype(BF).reshape(16, 16, wide)
            send[a][0, 0, :, :, cols] = rows
            recv[a][0, 0, 0, :, cols] = rows[0]
        split_copies(0, part, send, recv, ds, dr, 1)
    for n, half in ((0, 1), (1, 0), (1, 1)):
        for a in AXES:
            if n == 0:
                b_copies[a, 3, 0].wait_recv()
                b_copies[a, 2, 0].wait_recv()
                b_copies[a, 2, 1].wait_recv()
            rows = dot(
                lhs_s[2 * a + half, 256 * n : 256 * n + 256, :],
                lines[a][2 * half : 2 * half + 2].reshape(256, WIDTHS[a]),
            ).astype(BF).reshape(16, 16, WIDTHS[a])
            send[a][n, half] = rows
            if n == 0:
                recv[a][0, half, 0] = rows[0]
        plane_copies(half, n, send, recv, ds, dr, 1)

    l_cg.wait()
    l_cu.wait()
    l_cdn.wait()
    nrm = jnp.concatenate([lines[a][0] for a in AXES], axis=1)
    hidden = (silu(dot(nrm, cg_s[...])) * dot(nrm, cu_s[...])).astype(BF)
    shared_s[...] = dot(hidden, cdn_s[...])

    def row_of(a, q):
        d1, d2 = plane_split((q >> 4) & 15)
        d = ((q >> 8) & 1) * 2 + ((q >> 3) & 1)
        dz, dy, dx = ((d1, d2, d), (d1, d, d2), (d, d1, d2))[a]
        return ((q >> 2) & 1) * 256 + (dz * 16 + dy * 4 + dx) * 4 + (q & 3)

    down = lax.broadcasted_iota(I32, (512, 512), 0)
    over = lax.broadcasted_iota(I32, (512, 512), 1)
    for a in AXES:
        pick_s[a] = (down == row_of(a, over)).astype(F32).astype(BF)
        place_s[a] = (over == row_of(a, down)).astype(F32).astype(BF)
    q_index = lax.broadcasted_iota(I32, (128, 512), 1)
    blank = jnp.zeros((120, 128), F32)
    for a in AXES:
        expert = expert_of(a, q_index >> 8, (q_index >> 4) & 15, (q_index >> 2) & 1).astype(F32)
        for d in range(4):
            info = jnp.concatenate([rt_s[4 * a + d if d else 0], blank], axis=0).T
            weight = jnp.zeros((128, 512), F32)
            match = jnp.zeros((128, 512), F32)
            for j in range(4):
                hit = expert == info[:, j : j + 1]
                match = jnp.where(hit, 1.0, match)
                weight = jnp.where(hit, info[:, 4 + j : 5 + j], weight)
            rank = dot(lower, match.astype(BF))
            live = (rank == (q_index & 3).astype(F32)) & (((q_index >> 3) & 1) == d % 2)
            rows = slice(128 * (d % 2), 128 * (d % 2) + 128)
            cw_s[2 * a + d // 2, rows, :] = jnp.where(live, weight, 0.0).astype(BF)

    l_wg.wait()
    l_wu.wait()
    l_wd.wait()
    for n in (0, 1):
        picked = []
        for a in AXES:
            for half in (0, 1):
                if (n, half) == (0, 0):
                    out_wait(a, 0).wait_recv()
                    out_wait(a, 1).wait_recv()
                else:
                    plane_wait(a, half, n, send, recv, ds, dr).wait_recv()
            picked.append(dot(pick_s[a], recv[a][n].reshape(512, WIDTHS[a])).astype(BF))
        acts = []
        for j in (0, 1):
            rows = jnp.concatenate([p[256 * j : 256 * j + 256] for p in picked], axis=1)
            acts.append((silu(dot(rows, wg_s[j])) * dot(rows, wu_s[j])).astype(BF))
        for half in (1, 0):
            for a in AXES:
                rows = slice(256 * half, 256 * half + 256)
                both = jnp.concatenate(
                    [dot(place_s[a, rows, 256 * j : 256 * j + 256], acts[j]).astype(BF) for j in (0, 1)],
                    axis=1,
                )
                cols = slice(STARTS[a], STARTS[a] + WIDTHS[a])
                done = jnp.concatenate([wd_s[0, :, cols], wd_s[1, :, cols]], axis=0)
                done = dot(both, done).astype(BF).reshape(16, 16, WIDTHS[a])
                ret[a][n, half] = done
                if n == 0:
                    back[a][0, half, 0] = done[0]
            if (n, half) == (1, 0):
                split_copies(1, 0, ret, back, es, er, -1)
            else:
                plane_copies(half, n, ret, back, es, er, -1)

    for one in b_copies.values():
        one.wait_send()
    p_copies = []

    def plane_sum(a, half, cols):
        return sum(
            dot(
                cw_s[2 * a + half, :, 256 * n : 256 * n + 256],
                back[a][n, half, :, :, cols].reshape(256, cols.stop - cols.start),
            )
            for n in (0, 1)
        )

    for a in AXES:
        for n in (0, 1):
            plane_wait(a, 1, n, ret, back, es, er).wait_recv()
        sum_a = plane_sum(a, 1, slice(0, WIDTHS[a]))
        lines[a][2] = sum_a[0:128].astype(BF)
        third_s[:, STARTS[a] : STARTS[a] + WIDTHS[a]] = sum_a[128:256]
        for part, toward in ((0, 3), (1, 1)):
            one = relay(
                a, part, lines[a].at[2], sums[a].at[1], ps.at[8 * a + part], pr.at[8 * a + part],
                toward,
            )
            one.start()
            p_copies.append(one)
    relayed = list(p_copies)
    split_copies(1, 1, ret, back, es, er, -1)
    for part in (0, 1):
        for a in AXES:
            cols = columns(a, part)
            whole = slice(STARTS[a] + cols.start, STARTS[a] + cols.stop)
            if part == 0:
                plane_wait(a, 0, 0, ret, back, es, er).wait_recv()
            last_wait(a, part).wait_recv()
            sum_a = plane_sum(a, 0, cols)
            shared_s[:, whole] += sum_a[0:128]
            value = sum_a[128:256]
            if part == 0:
                relayed[2 * a].wait_recv()
                value = value + sums[a][1, :, cols].astype(F32)
            lines[a][1, :, cols] = value.astype(BF)
            one = relay(
                a, part, lines[a].at[1], sums[a].at[0], ps.at[8 * a + 2 + part],
                pr.at[8 * a + 2 + part], 3,
            )
            one.start()
            p_copies.append(one)
        if part == 0:
            for a in AXES:
                cols = slice(FIRST[a], WIDTHS[a])
                relayed[2 * a + 1].wait_recv()
                value = third_s[:, STARTS[a] : STARTS[a] + WIDTHS[a]]
                lines[a][3, :, 0 : FIRST[a]] = value[:, 0 : FIRST[a]].astype(BF)
                lines[a][3, :, cols] = (value[:, cols] + sums[a][1, :, cols].astype(F32)).astype(BF)
                one = pltpu.make_async_remote_copy(
                    src_ref=lines[a].at[3], dst_ref=sums[a].at[2],
                    send_sem=ps.at[8 * a + 4], recv_sem=pr.at[8 * a + 4],
                    device_id=along(a, 1), device_id_type=MESH,
                )
                one.start()
                p_copies.append(one)
    for one in p_copies:
        if not any(one is r for r in relayed):
            one.wait_recv()
    for a in AXES:
        cols = slice(STARTS[a], STARTS[a] + WIDTHS[a])
        value = mid_s[:, cols].astype(F32) + shared_s[:, cols]
        value = value + sums[a][0].astype(F32) + sums[a][2].astype(F32)
        out_ref[:, cols] = value.astype(BF)
    for one in p_copies:
        one.wait_send()
    for n in (0, 1):
        for half in (0, 1):
            for a in AXES:
                if (n, half) == (0, 0):
                    out_wait(a, 0).wait_send()
                    out_wait(a, 1).wait_send()
                else:
                    plane_wait(a, half, n, send, recv, ds, dr).wait_send()
                if (n, half) == (1, 0):
                    last_wait(a, 0).wait_send()
                    last_wait(a, 1).wait_send()
                else:
                    plane_wait(a, half, n, ret, back, es, er).wait_send()


def on_device(
    queries, key_matrix, value_matrix, channel_decay_input, head_decay_offset, output_gate_input,
    head_norm_gain, residual, mixer_output_weight, expert_norm_gain, routes, chosen_router_scores,
    routed_gate_weight, routed_up_weight, routed_down_weight, common_gate_weight,
    common_up_weight, common_down_weight,
):
    any_ = pl.BlockSpec(memory_space=pl.ANY)
    vm = pl.BlockSpec(memory_space=pltpu.VMEM)
    dma = pltpu.SemaphoreType.DMA
    V = pltpu.VMEM
    return pl.pallas_call(
        kernel,
        out_shape=jax.ShapeDtypeStruct((128, 2048), BF),
        in_specs=[
            any_, any_, any_, any_, vm, any_, vm, any_, any_, vm,
            vm, vm, any_, any_, any_, any_, any_, any_,
        ],
        out_specs=vm,
        scratch_shapes=[
            V((512, 128), BF), V((512, 128), BF), V((512, 256), BF), V((512, 128), BF),
            V((512, 256), BF), V((128, 2048), BF), V((1024, 2048), BF),
            V((2, 2048, 512), BF), V((2, 2048, 512), BF), V((2, 512, 2048), BF),
            V((2048, 512), BF), V((2048, 512), BF), V((512, 2048), BF),
            V((144, 128), BF), V((144, 128), BF), V((NY, 144, 128), BF), V((NZ, 144, 128), BF),
            V((2, 512, 128), F32), V((512, 128), BF), V((4, 128, 256), BF), V((4, 128, 256), BF),
            V((128, 2048), BF), V((128, 2048), F32), V((128, 2048), F32),
            V((12, 8, 128), F32), V((6, 512, 256), BF), V((6, 256, 512), BF),
            V((3, 512, 512), BF), V((3, 512, 512), BF),
            *[V((4, 128, w), BF) for w in WIDTHS], *[V((3, 128, w), BF) for w in WIDTHS],
            *[V((2, 2, 16, 16, w), BF) for _ in range(4) for w in WIDTHS],
            dma((13,)), dma, dma, dma((4,)), dma((4,)), dma((4,)), dma((4,)), dma((4,)), dma((4,)),
            dma((12,)), dma((12,)), dma((24,)), dma((24,)), *[dma((15,)) for _ in range(4)],
            dma((24,)), dma((24,)),
        ],
        compiler_params=pltpu.CompilerParams(
            collective_id=0, has_side_effects=True, vmem_limit_bytes=62 * 1024 * 1024
        ),
        name="layer",
    )(
        queries, key_matrix, value_matrix, channel_decay_input, head_decay_offset.T,
        output_gate_input, head_norm_gain.reshape(1, 128), residual, mixer_output_weight,
        expert_norm_gain.reshape(1, 2048), routes.T, chosen_router_scores.T, routed_gate_weight,
        routed_up_weight, routed_down_weight, common_gate_weight, common_up_weight,
        common_down_weight,
    )


def solution(mesh):
    both = ("sp", "tp")
    split, rows, rep = P("sp", "tp"), P(both, None), P()
    return jax.shard_map(
        on_device,
        mesh=mesh,
        in_specs=(
            split, split, split, split, split, split, rep, rows, rep, rep, rows, rows,
            P(both, None, None), P(both, None, None), P(both, None, None), rep, rep, rep,
        ),
        out_specs=rows,
        check_vma=False,
    )
```
